256 devices in a mesh: sp: 32 (over z, x), tp: 8 (over y, core).
Axes of the slice: x: 4, y: 4, z: 8, core: 2. Of those that a mesh axis runs over, the one named last changes fastest.
Arguments:
- queries: bfloat16 [16384, 1024], P('sp', 'tp'), may hold values from -5.5 to 5.5
- key_vectors: bfloat16 [16384, 1024], P('sp', 'tp'), may hold values from -5.5 to 5.5
- latents: bfloat16 [16384, 2048], P('sp', 'tp'), may hold values from -6 to 6
- w_value: bfloat16 [2048, 1024], P(None, 'tp'), may hold values from -0.125 to 0.125
- log_sums: float32 [16384, 16], P('sp', 'tp'), as said below
- out_pair: bfloat16 [16384, 2048], P('sp', 'tp'), may hold values from -6 to 6
- cotangent: bfloat16 [16384, 1024], P('sp', 'tp'), may hold values from -6 to 6
- lambdas: float32 [8], P('tp'), may hold values from 0.3 to 0.8
- out_gain: float32 [128], replicated, may hold values from 0.1 to 1.9
Outputs:
- query_grad: float32 [16384, 1024], P('sp', 'tp')
- key_grad: float32 [16384, 1024], P('sp', 'tp')
- value_grad: float32 [16384, 1024], P('sp', 'tp')
- weight_grad: float32 [2048, 1024], P('sp', 'tp')
The draws below stay inside these ranges and needn't reach their ends.
Inputs may be any that keep to these rules, and one draw needn't show every extreme that they name: `log_sums`: each entry is the logarithm of the sum of exp(scores_c[t, s]) over s <= t for its row t, head h and map c.
All inputs are finite; a program needn't handle non-finite values.
Results may differ from the reference program's by a relative error of at most 0.008.
Values may be sent and summed in bfloat16 or wider, within the bound.
A program may use at most 64 MiB of HBM per device.

```python
import jax
import jax.numpy as jnp
from jax import lax

TOK_DEV = 512
D = 2048
HEADS = 8
QK = 64
VALUE = 128
SEQ = 16384


def pair_draw(key):
    arr_shape = (SEQ, HEADS * 2 * QK)
    key_query = jax.random.fold_in(key, 501)
    key_keys = jax.random.fold_in(key, 502)
    query_vals = jnp.clip(1.3 * jax.random.normal(key_query, arr_shape, jnp.float32), -5.5, 5.5)
    key_vals = jnp.clip(1.3 * jax.random.normal(key_keys, arr_shape, jnp.float32), -5.5, 5.5)
    return (query_vals.astype(jnp.bfloat16), key_vals.astype(jnp.bfloat16))


def draw_queries(key, part):
    return pair_draw(key)[0]


def draw_key_vectors(key, part):
    return pair_draw(key)[1]


def draw_log_sums(key, part):
    query_vals, key_vals = pair_draw(key)
    query_wide = query_vals.astype(jnp.float32).reshape(SEQ, HEADS * 2, QK)
    key_wide = key_vals.astype(jnp.float32).reshape(SEQ, HEADS * 2, QK)
    factor = QK ** (-0.5)
    key_pos = jnp.arange(SEQ, dtype=jnp.int32)

    def per_block(block_idx):
        begin_row = (block_idx * TOK_DEV).astype(jnp.int32)
        query_block = lax.dynamic_slice_in_dim(query_wide, begin_row, TOK_DEV, 0)
        query_pos = begin_row + jnp.arange(TOK_DEV, dtype=jnp.int32)
        visible = key_pos[None, :] <= query_pos[:, None]

        def per_map(map_idx):
            query_map = lax.dynamic_index_in_dim(query_block, map_idx, 1, keepdims=False)
            key_map = lax.dynamic_index_in_dim(key_wide, map_idx, 1, keepdims=False)
            scores = jnp.dot(query_map, key_map.T, precision=lax.Precision.HIGHEST) * factor
            masked = jnp.where(visible, scores, -jnp.inf)
            largest = jnp.max(masked, axis=1)
            return largest + jnp.log(jnp.sum(jnp.where(visible, jnp.exp(masked - largest[:, None]), 0.0), axis=1))
        return lax.map(per_map, jnp.arange(HEADS * 2, dtype=jnp.int32)).T
    result = lax.map(per_block, jnp.arange(SEQ // TOK_DEV, dtype=jnp.int32))
    return result.reshape(SEQ, HEADS * 2).astype(jnp.float32)


def with_spikes(values, rng, source, target, parts, factor):
    owner, partner = [(jnp.arange(values.shape[axis_at]) // (values.shape[axis_at] // parts)).reshape([-1 if axis == axis_at else 1 for axis in range(values.ndim)]) for axis_at in (source, target)]
    chosen = jax.random.permutation(rng, parts)[partner]
    strong = (owner == chosen) | (owner == (partner + parts // 2) % parts)
    return jnp.where(strong, factor * values, values)


def levels(own_key, extent, split, low, high):
    factor_of, own = 1.0, jax.random.fold_in(own_key, 6)
    for axis_at, shards_of in split:
        steps = jnp.exp(jax.random.uniform(jax.random.fold_in(own, axis_at), (shards_of,), jnp.float32, low / len(split), high / len(split)))
        factor_of = factor_of * jnp.repeat(steps, extent[axis_at] // shards_of).reshape([-1 if axis == axis_at else 1 for axis in range(len(extent))])
    return factor_of


def scatter_about(key, dims, width, bound, split=(), kind=jnp.bfloat16):
    values = width * jax.random.normal(key, dims, jnp.float32)
    if split:
        values = values * levels(key, dims, split, -0.22, 0.18)
    return jnp.clip(values, -bound, bound).astype(kind)


def gaussian_with(rng, extent, deviation, bound, split, heavy, kind=jnp.bfloat16):
    drawn = deviation * jax.random.normal(rng, extent, jnp.float32)
    if split:
        drawn = drawn * levels(rng, extent, split, -0.22, 0.18)
    return jnp.clip(with_spikes(drawn, jax.random.fold_in(rng, 3), *heavy), -bound, bound).astype(kind)


def setup_inputs(seed: int = 0) -> dict:
    keys = jax.random.split(jax.random.key(seed), 10)
    queries = draw_queries(jax.random.fold_in(keys[9], 71), 0)
    key_vectors = draw_key_vectors(jax.random.fold_in(keys[9], 71), 0)
    latents = scatter_about(keys[2], (SEQ, D), 1.0, 6.0, ((0, 32), (1, 8)))
    w_value = scatter_about(keys[3], (D, HEADS * VALUE), D ** -0.5, 0.125, ((1, 8),))
    log_sums = draw_log_sums(jax.random.fold_in(keys[9], 71), 0)
    out_pair = scatter_about(keys[5], (SEQ, HEADS * 2 * VALUE), 1.0, 6.0, ((0, 32), (1, 8)))
    cotangent = gaussian_with(keys[6], (SEQ, HEADS * VALUE), 1.0, 6.0, ((0, 32), (1, 8)), (0, 1, 32, 2.75))
    lambdas = jnp.clip(0.3 + 0.5 * jax.random.uniform(keys[7], (HEADS,), jnp.float32) ** levels(keys[7], (HEADS,), ((0, 8),), -0.2, 0.2), 0.3, 0.8)
    out_gain = jnp.clip(1.0 + 0.18 * jax.random.normal(keys[8], (VALUE,), jnp.float32), 0.1, 1.9)
    return dict(queries=queries, key_vectors=key_vectors, latents=latents, w_value=w_value, log_sums=log_sums, out_pair=out_pair, cotangent=cotangent, lambdas=lambdas, out_gain=out_gain)


norm_floor = 0.25

def head_cotangent(out_pair, cotangent, lambdas, out_gain):
    tok_rows = out_pair.shape[0]
    head_count = lambdas.shape[0]
    out_maps = out_pair.astype(jnp.float32).reshape(tok_rows, head_count, 2, -1)
    lam_cols = lambdas[None, :, None]
    merged = out_maps[:, :, 0] - lam_cols * out_maps[:, :, 1]
    inv_norm = lax.rsqrt(lax.optimization_barrier(jnp.mean(merged * merged, axis=-1, keepdims=True)) + norm_floor)
    scaled = cotangent.astype(jnp.float32).reshape(merged.shape) * out_gain
    inner_dot = lax.optimization_barrier(jnp.mean(scaled * merged, axis=-1, keepdims=True))
    out_grad = (inv_norm * scaled - merged * (inv_norm * inv_norm * inv_norm) * inner_dot).astype(jnp.bfloat16)
    grad_wide = out_grad.astype(jnp.float32)
    first_map = lax.optimization_barrier(jnp.sum(grad_wide * out_maps[:, :, 0], axis=-1))
    second_map = -lambdas[None, :] * lax.optimization_barrier(jnp.sum(grad_wide * out_maps[:, :, 1], axis=-1))
    return (out_grad, jnp.stack([first_map, second_map], axis=-1))

def block_terms(query_block, key_block, value_block, grad_block, log_block, term_block, lambdas, query_pos, key_pos):
    factor = query_block.shape[-1] ** (-0.5)
    scores = jnp.einsum('qhcd,khcd->hcqk', query_block.astype(jnp.float32), key_block.astype(jnp.float32)) * factor
    visible = key_pos[None, :] <= query_pos[:, None]
    shifted = scores - jnp.transpose(log_block, (1, 2, 0))[..., None]
    softmax_maps = jnp.where(visible, jnp.exp(shifted), 0.0)
    value_dot = jnp.einsum('qhe,khe->hqk', grad_block.astype(jnp.float32), value_block.astype(jnp.float32))
    lam_cols = lambdas[:, None, None]
    weights = (softmax_maps[:, 0] - lam_cols * softmax_maps[:, 1]).astype(jnp.bfloat16)
    term_cols = jnp.transpose(term_block, (1, 2, 0))
    first_map = softmax_maps[:, 0] * (value_dot - term_cols[:, 0, :, None])
    second_map = softmax_maps[:, 1] * (-lam_cols * value_dot - term_cols[:, 1, :, None])
    dscore = (jnp.stack([first_map, second_map], axis=1) * factor).astype(jnp.bfloat16)
    return (weights, dscore)

def reference(queries, key_vectors, latents, w_value, log_sums, out_pair, cotangent, lambdas, out_gain):
    values = jnp.dot(latents, w_value, preferred_element_type=jnp.float32).astype(jnp.bfloat16)
    out_grad, row_terms = head_cotangent(out_pair, cotangent, lambdas, out_gain)
    query_heads = jnp.moveaxis(queries.reshape(SEQ, HEADS, 1, 2, QK), 1, 0)
    key_heads = jnp.moveaxis(key_vectors.reshape(SEQ, HEADS, 1, 2, QK), 1, 0)
    value_heads = jnp.moveaxis(values.reshape(SEQ, HEADS, 1, VALUE), 1, 0)
    grad_heads = jnp.moveaxis(out_grad.reshape(SEQ, HEADS, 1, VALUE), 1, 0)
    log_heads = jnp.moveaxis(log_sums.reshape(SEQ, HEADS, 1, 2), 1, 0)
    term_heads = jnp.moveaxis(row_terms.reshape(SEQ, HEADS, 1, 2), 1, 0)
    lam_heads = lambdas.reshape(HEADS, 1)
    key_pos = jnp.arange(SEQ, dtype=jnp.int32)

    def one_head(inputs):
        query_head, key_head, value_head, grad_head, log_head, term_head, lam_head = inputs

        def one_block(partial_value, block_idx):
            begin_row = (block_idx * TOK_DEV).astype(jnp.int32)
            query_block = lax.dynamic_slice_in_dim(query_head, begin_row, TOK_DEV, 0)
            grad_block = lax.dynamic_slice_in_dim(grad_head, begin_row, TOK_DEV, 0)
            log_block = lax.dynamic_slice_in_dim(log_head, begin_row, TOK_DEV, 0)
            term_block = lax.dynamic_slice_in_dim(term_head, begin_row, TOK_DEV, 0)
            query_pos = begin_row + jnp.arange(TOK_DEV, dtype=jnp.int32)
            weights, dscore = block_terms(query_block, key_head, value_head, grad_block, log_block, term_block, lam_head, query_pos, key_pos)
            score_wide = dscore.astype(jnp.float32)
            query_part = jnp.einsum('hcqk,khcd->qhcd', score_wide, key_head.astype(jnp.float32))
            key_part = jnp.einsum('hcqk,qhcd->khcd', score_wide, query_block.astype(jnp.float32))
            value_part = jnp.einsum('hqk,qhe->khe', weights.astype(jnp.float32), grad_block.astype(jnp.float32))
            return ((partial_value[0] + key_part, partial_value[1] + value_part), query_part)
        start_sums = (jnp.zeros(key_head.shape, jnp.float32), jnp.zeros(value_head.shape, jnp.float32))
        sums, query_parts = lax.scan(one_block, start_sums, jnp.arange(SEQ // TOK_DEV, dtype=jnp.int32))
        return (query_parts.reshape(query_head.shape), sums[0], sums[1])
    query_grad, key_grad, value_grad = lax.map(one_head, (query_heads, key_heads, value_heads, grad_heads, log_heads, term_heads, lam_heads))
    query_grad = jnp.moveaxis(query_grad, 0, 1).reshape(SEQ, HEADS * 2 * QK)
    key_grad = jnp.moveaxis(key_grad, 0, 1).reshape(SEQ, HEADS * 2 * QK)
    value_grad = jnp.moveaxis(value_grad, 0, 1).reshape(SEQ, HEADS * VALUE)
    value_narrow = value_grad.astype(jnp.bfloat16)
    weight_grad = jnp.dot(latents.T, value_narrow, preferred_element_type=jnp.float32)
    return (query_grad, key_grad, value_grad, weight_grad)
```

```python
import functools
import math

import jax
import jax.numpy as jnp
import numpy as np
from jax import lax
from jax.experimental import pallas as pl
from jax.experimental.pallas import tpu as pltpu
from jax.sharding import Mesh, PartitionSpec as P

norm_floor = 0.25
log2_e = math.log2(math.e)
f32 = jnp.float32
bf16 = jnp.bfloat16
rows_by_rows = (((1,), (1,)), ((), ()))
rows_by_cols = (((1,), (0,)), ((), ()))
cols_by_cols = (((0,), (0,)), ((), ()))


def head_cotangent(out_pair, cotangent, lam, out_gain):
    first_out = out_pair[:, :128].astype(f32)
    second_out = out_pair[:, 128:].astype(f32)
    merged = first_out - lam * second_out
    inv_norm = lax.rsqrt(jnp.mean(merged * merged, axis=-1, keepdims=True) + norm_floor)
    scaled = cotangent.astype(f32) * out_gain
    inner_dot = jnp.mean(scaled * merged, axis=-1, keepdims=True)
    out_grad = (inv_norm * scaled - merged * (inv_norm * inv_norm * inv_norm) * inner_dot).astype(bf16)
    wide = out_grad.astype(f32)
    return out_grad, jnp.sum(wide * first_out, axis=-1), jnp.sum(wide * second_out, axis=-1)


def attention_kernel(place, query_ref, row_ref, key_ref, dq_ref, dk_ref, dv_ref, *, key_len, tok_len):
    low, col, half = place[0], place[1], place[2]
    dq_ref[...] = jnp.zeros_like(dq_ref)
    dk_ref[...] = jnp.zeros_like(dk_ref)
    dv_ref[...] = jnp.zeros_like(dv_ref)
    first_lanes = lax.broadcasted_iota(jnp.int32, (1, 128), 1) < 64
    first_count = 8 - low

    def split(x):
        zero = jnp.zeros_like(x)
        return jnp.where(first_lanes, x, zero), jnp.where(first_lanes, zero, x)

    def tile(step, masked):
        second = step >= first_count
        group = jnp.where(second, 1, 0)
        block = jnp.where(second, 7 - low + (step - first_count), low + step)
        for tok in range(0, 512, tok_len):
            toks = slice(tok, tok + tok_len)
            query = query_ref[block, toks, 0:128]
            grad = query_ref[block, toks, 128:256]
            query_0, query_1 = split(query)
            log_0, log_1 = row_ref[block, 0:1, toks], row_ref[block, 1:2, toks]
            term_0, term_1 = row_ref[block, 2:3, toks], row_ref[block, 3:4, toks]
            for key in range(0, 1024, key_len):
                keys = slice(key, key + key_len)
                key_0, key_1 = split(key_ref[group, keys, 0:128])
                value = key_ref[group, keys, 128:256]
                score_0 = lax.dot_general(key_0, query, rows_by_rows, preferred_element_type=f32)
                score_1 = lax.dot_general(key_1, query, rows_by_rows, preferred_element_type=f32)
                dot = lax.dot_general(value, grad, rows_by_rows, preferred_element_type=f32)
                map_0 = jnp.exp2(score_0 * (log2_e / 8) - log_0)
                map_1 = jnp.exp2(score_1 * (log2_e / 8) - log_1)
                if masked:
                    row = lax.broadcasted_iota(jnp.int32, (key_len, 1), 0) + key
                    key_pos = (row // 256 - col) * 512 + half * 256 + row % 256
                    tok_pos = lax.broadcasted_iota(jnp.int32, (1, tok_len), 1) + tok
                    visible = key_pos <= tok_pos
                    map_0 = jnp.where(visible, map_0, 0.0)
                    map_1 = jnp.where(visible, map_1, 0.0)
                grad_0 = (map_0 * (dot - term_0)).astype(bf16)
                grad_1 = (map_1 * (term_1 - dot)).astype(bf16)
                mixed = (map_0 - map_1).astype(bf16)
                dk_ref[group, keys, :] += lax.dot_general(
                    grad_0, query_0, rows_by_cols, preferred_element_type=f32
                ) + lax.dot_general(grad_1, query_1, rows_by_cols, preferred_element_type=f32)
                dv_ref[group, keys, :] += lax.dot_general(
                    mixed, grad, rows_by_cols, preferred_element_type=f32
                )
                dq_ref[block, toks, :] += lax.dot_general(
                    grad_0, key_0, cols_by_cols, preferred_element_type=f32
                ) + lax.dot_general(grad_1, key_1, cols_by_cols, preferred_element_type=f32)

    def one_step(step, carry):
        diagonal = (step == 0) | (step == first_count)
        pl.when(diagonal)(lambda: tile(step, True))
        pl.when(jnp.logical_not(diagonal))(lambda: tile(step, False))
        return carry

    lax.fori_loop(0, 9, one_step, 0)


def attention(place, queries, rows, keys):
    vmem = pl.BlockSpec(memory_space=pltpu.VMEM)
    return pl.pallas_call(
        functools.partial(attention_kernel, key_len=512, tok_len=256),
        out_shape=(
            jax.ShapeDtypeStruct((8, 512, 128), f32),
            jax.ShapeDtypeStruct((2, 1024, 128), f32),
            jax.ShapeDtypeStruct((2, 1024, 128), f32),
        ),
        in_specs=[pl.BlockSpec(memory_space=pltpu.SMEM), vmem, vmem, vmem],
        out_specs=[vmem, vmem, vmem],
        compiler_params=pltpu.CompilerParams(vmem_limit_bytes=60 * 1024 * 1024),
        cost_estimate=pl.CostEstimate(flops=9 * 1024 * 512 * 2048, bytes_accessed=8 << 20, transcendentals=0),
        name="attention",
    )(place, queries, rows, keys)


def per_device(queries, key_vectors, latents, w_value, log_sums, out_pair, cotangent, lambdas, out_gain):
    z, x = lax.axis_index("z"), lax.axis_index("x")
    lam = lambdas[0]
    low = jnp.minimum(z, 7 - z)
    half = jnp.where(z < 4, 0, 1)
    mirror = [(i, 7 - i) for i in range(8)]

    out_grad, first_term, second_term = head_cotangent(out_pair, cotangent, lam, out_gain)
    rows = jnp.stack(
        [log_sums[:, 0] * log2_e, log_sums[:, 1] * log2_e - jnp.log2(lam), first_term, second_term]
    )
    query_all = lax.all_gather(jnp.concatenate([queries, out_grad], axis=1), "z")
    row_all = lax.all_gather(rows, "z")

    latents_all = lax.all_gather(latents, ("y", "core"), axis=1, tiled=True)
    values = jnp.dot(latents_all, w_value, preferred_element_type=f32).astype(bf16)
    pair = jnp.concatenate([key_vectors, values], axis=1).reshape(2, 256, 256)
    kept = lax.dynamic_index_in_dim(pair, half, 0, keepdims=False)
    given = lax.dynamic_index_in_dim(pair, 1 - half, 0, keepdims=False)
    came = lax.ppermute(given, "z", mirror)
    upper = z >= 4
    key_two = jnp.stack([jnp.where(upper, came, kept), jnp.where(upper, kept, came)])
    key_all = lax.all_gather(key_two, "x", axis=1).reshape(2, 1024, 256)

    place = jnp.stack([low, x, half]).astype(jnp.int32)
    dq, dk, dv = attention(place, query_all, row_all, key_all)

    query_grad = lax.psum_scatter(dq, "z", scatter_dimension=0) * 0.125
    both = jnp.concatenate([dk * 0.125, dv], axis=-1).reshape(2, 4, 256, 256)
    own = lax.psum_scatter(both, "x", scatter_dimension=1)
    kept = jnp.where(upper, own[1], own[0])
    given = jnp.where(upper, own[0], own[1])
    came = lax.ppermute(given, "z", mirror)
    whole = jnp.concatenate([jnp.where(upper, came, kept), jnp.where(upper, kept, came)])
    key_grad, value_grad = whole[:, :128], whole[:, 128:]
    partial = lax.dot_general(
        latents_all, value_grad.astype(bf16), cols_by_cols, preferred_element_type=f32
    )
    weight_grad = lax.psum_scatter(partial, ("z", "x"), scatter_dimension=0, tiled=True)
    return query_grad, key_grad, value_grad, weight_grad


def solution(mesh):
    grid = Mesh(mesh.devices.reshape(8, 4, 4, 2), ("z", "x", "y", "core"))
    sp, tp = ("z", "x"), ("y", "core")
    return jax.shard_map(
        per_device,
        mesh=grid,
        in_specs=(
            P(sp, tp),
            P(sp, tp),
            P(sp, tp),
            P(None, tp),
            P(sp, tp),
            P(sp, tp),
            P(sp, tp),
            P(tp),
            P(),
        ),
        out_specs=(P(sp, tp), P(sp, tp), P(sp, tp), P(sp, tp)),
        check_vma=False,
    )
```

```python
import functools
import math

import jax
import jax.numpy as jnp
import numpy as np
from jax import lax
from jax.experimental import pallas as pl
from jax.experimental.pallas import tpu as pltpu
from jax.sharding import Mesh, PartitionSpec as P

norm_floor = 0.25
log2_e = math.log2(math.e)
f32 = jnp.float32
bf16 = jnp.bfloat16
rows_by_rows = (((1,), (1,)), ((), ()))
rows_by_cols = (((1,), (0,)), ((), ()))
cols_by_cols = (((0,), (0,)), ((), ()))


def head_cotangent(out_pair, cotangent, lam, out_gain):
    first_out = out_pair[:, :128].astype(f32)
    second_out = out_pair[:, 128:].astype(f32)
    merged = first_out - lam * second_out
    inv_norm = lax.rsqrt(jnp.mean(merged * merged, axis=-1, keepdims=True) + norm_floor)
    scaled = cotangent.astype(f32) * out_gain
    inner_dot = jnp.mean(scaled * merged, axis=-1, keepdims=True)
    out_grad = (inv_norm * scaled - merged * (inv_norm * inv_norm * inv_norm) * inner_dot).astype(bf16)
    wide = out_grad.astype(f32)
    return out_grad, jnp.sum(wide * first_out, axis=-1), jnp.sum(wide * second_out, axis=-1)


mesh_ids = pl.DeviceIdType.MESH


class Sender:
    def __init__(self, send_sems, recv_sems):
        self.send_sems, self.recv_sems, self.copies = send_sems, recv_sems, {}

    def start(self, name, source, target, device):
        place = len(self.copies)
        copy = pltpu.make_async_remote_copy(
            src_ref=source,
            dst_ref=target,
            send_sem=self.send_sems.at[place],
            recv_sem=self.recv_sems.at[place],
            device_id=device,
            device_id_type=mesh_ids,
        )
        self.copies[name] = copy
        copy.start()

    def arrived(self, name):
        self.copies[name].wait_recv()

    def finish(self):
        for copy in self.copies.values():
            copy.wait_send()


def greet(devices):
    barrier = pltpu.get_barrier_semaphore()
    for device in devices:
        pl.semaphore_signal(barrier, inc=1, device_id=device, device_id_type=mesh_ids)
    pl.semaphore_wait(barrier, len(devices))


def gather_kernel(
    query_ref, row_ref, latent_ref, weight_ref, key_ref,
    query_all, row_all, latent_all, key_all, value_all,
    value_own, send_sems, recv_sems,
):
    z, x, y, core = (lax.axis_index(name) for name in ("z", "x", "y", "core"))
    up, down = {"z": lax.rem(z + 1, 8)}, {"z": lax.rem(z + 7, 8)}
    mirror = {"z": 7 - z}
    right, left = {"x": lax.rem(x + 1, 4)}, {"x": lax.rem(x + 3, 4)}
    ahead, behind = {"y": lax.rem(y + 1, 4)}, {"y": lax.rem(y + 3, 4)}
    partner = {"core": 1 - core}
    greet([up, down, mirror, right, left, ahead, behind, partner])
    sender = Sender(send_sems, recv_sems)
    start, arrived = sender.start, sender.arrived
    group = jnp.where(z < 4, 0, 1)
    half = group
    halves = (pl.ds(0, 256), pl.ds(256, 256))

    def latent_slot(step, part):
        slot = lax.rem(y + step + 4, 4) * 2 + core
        return latent_all.at[slot, halves[part]]

    def latent_to_partner(step, part):
        start(("pair", step, part), latent_slot(step, part), latent_slot(step, part), partner)

    def query_slot(step, part):
        return query_all.at[lax.rem(z + step + 8, 8), halves[part]]

    def send_query(way, hops, part):
        device, sign = (up, -1) if way == "up" else (down, 1)
        source = query_ref.at[halves[part]] if hops == 0 else query_slot(sign * hops, part)
        start((way, hops, part), source, query_slot(sign * hops, part), device)

    def send_rows(way, hops):
        device, sign = (up, -1) if way == "up" else (down, 1)
        slot = row_all.at[lax.rem(z + sign * hops + 8, 8)]
        start((way, hops, "rows"), row_ref if hops == 0 else slot, slot, device)

    def pass_query(hops, step):
        for way, part in (("up", step), ("down", 1 - step)):
            arrived((way, hops, part))
            if hops < 2 or (hops == 2 and step == 0):
                send_query(way, hops + 1, part)
            if step == 0 and hops < (4 if way == "up" else 3):
                arrived((way, hops, "rows"))
                if hops < (3 if way == "up" else 2):
                    send_rows(way, hops + 1)

    def open_share(name, whole, target):
        start((name, "mirror"), whole.at[1 - half], target.at[group, x], mirror)
        start((name, "own", "right"), whole.at[half], target.at[group, x], right)
        start((name, "own", "left"), whole.at[half], target.at[group, x], left)

    def share_mirrored(name, target):
        arrived((name, "mirror"))
        slot = target.at[1 - group, x]
        start((name, "other", "left"), slot, slot, left)
        start((name, "other", "right"), slot, slot, right)

    def share_far(name, target):
        arrived((name, "own", "right"))
        slot = target.at[group, lax.rem(x + 3, 4)]
        start((name, "own", "far"), slot, slot, right)
        arrived((name, "other", "left"))
        slot = target.at[1 - group, lax.rem(x + 1, 4)]
        start((name, "other", "far"), slot, slot, left)

    def close_share(name):
        arrived((name, "own", "left"))
        arrived((name, "other", "right"))
        arrived((name, "own", "far"))
        arrived((name, "other", "far"))

    own_slot = y * 2 + core
    for way, part, device in (("ahead", 0, ahead), ("behind", 1, behind), ("ahead", 1, ahead), ("behind", 0, behind)):
        start((way, part), latent_ref.at[halves[part]], latent_all.at[own_slot, halves[part]], device)
    start("pair", latent_ref, latent_all.at[own_slot], partner)
    send_query("up", 0, 0)
    send_query("down", 0, 1)
    send_rows("up", 0)
    send_rows("down", 0)
    open_share("key", key_ref, key_all)
    send_query("up", 0, 1)
    send_query("down", 0, 0)
    latent_all[own_slot] = latent_ref[...]
    query_all[z] = query_ref[...]
    row_all[z] = row_ref[...]
    key_all[group, x] = key_ref[half]

    arrived(("ahead", 0))
    start(("ahead", "far"), latent_slot(-1, 0), latent_slot(-1, 0), ahead)
    latent_to_partner(-1, 0)
    arrived(("behind", 1))
    start(("behind", "far"), latent_slot(1, 1), latent_slot(1, 1), behind)
    latent_to_partner(1, 1)
    pass_query(0, 0)
    share_mirrored("key", key_all)
    arrived(("ahead", 1))
    latent_to_partner(-1, 1)
    arrived(("behind", 0))
    latent_to_partner(1, 0)
    pass_query(0, 1)
    share_far("key", key_all)
    arrived(("ahead", "far"))
    latent_to_partner(2, 0)
    arrived(("behind", "far"))
    latent_to_partner(2, 1)
    pass_query(1, 0)
    arrived("pair")
    for step in (-1, 1, 2):
        for part in (0, 1):
            arrived(("pair", step, part))
    total = jnp.zeros((512, 128), f32)
    for slot in range(8):
        total += jnp.dot(latent_all[slot], weight_ref[slot], preferred_element_type=f32)
    own = total.astype(bf16).reshape(2, 256, 128)
    value_own[...] = own
    open_share("value", value_own, value_all)
    value_all[group, x] = value_own[half]
    pass_query(1, 1)
    share_mirrored("value", value_all)
    pass_query(2, 0)
    share_far("value", value_all)
    pass_query(2, 1)
    close_share("key")
    close_share("value")
    pass_query(3, 0)
    sender.finish()


def gather(queries, rows, latents, w_value, keys):
    vmem = pl.BlockSpec(memory_space=pltpu.VMEM)
    return pl.pallas_call(
        gather_kernel,
        out_shape=(
            jax.ShapeDtypeStruct((8, 512, 256), bf16),
            jax.ShapeDtypeStruct((8, 8, 512), f32),
            jax.ShapeDtypeStruct((8, 512, 256), bf16),
            jax.ShapeDtypeStruct((2, 4, 256, 128), bf16),
            jax.ShapeDtypeStruct((2, 4, 256, 128), bf16),
        ),
        in_specs=[vmem] * 5,
        out_specs=[vmem] * 5,
        scratch_shapes=[
            pltpu.VMEM((2, 256, 128), bf16),
            pltpu.SemaphoreType.DMA((48,)),
            pltpu.SemaphoreType.DMA((48,)),
        ],
        compiler_params=pltpu.CompilerParams(
            collective_id=0, has_side_effects=True, vmem_limit_bytes=40 * 1024 * 1024
        ),
        name="gather",
    )(queries, rows, latents, w_value, keys)


def attention_kernel(place, query_ref, row_ref, key_ref, value_ref, dq_ref, dk_ref, dv_ref, *, key_len, tok_len):
    low, col, half = place[0], place[1], place[2]
    dq_ref[...] = jnp.zeros_like(dq_ref)
    dk_ref[...] = jnp.zeros_like(dk_ref)
    dv_ref[...] = jnp.zeros_like(dv_ref)
    first_lanes = lax.broadcasted_iota(jnp.int32, (1, 128), 1) < 64
    first_count = 8 - low

    def split(x):
        zero = jnp.zeros_like(x)
        return jnp.where(first_lanes, x, zero), jnp.where(first_lanes, zero, x)

    def tile(step, masked):
        second = step >= first_count
        group = jnp.where(second, 1, 0)
        block = jnp.where(second, 7 - low + (step - first_count), low + step)
        for tok in range(0, 512, tok_len):
            toks = slice(tok, tok + tok_len)
            query = query_ref[block, toks, 0:128]
            grad = query_ref[block, toks, 128:256]
            query_0, query_1 = split(query)
            log_0, log_1 = row_ref[block, 0:1, toks], row_ref[block, 1:2, toks]
            term_0, term_1 = row_ref[block, 2:3, toks], row_ref[block, 3:4, toks]
            for key in range(0, 1024, key_len):
                keys = slice(key, key + key_len)
                key_0, key_1 = split(key_ref[group, keys, :])
                value = value_ref[group, keys, :]
                score_0 = lax.dot_general(key_0, query, rows_by_rows, preferred_element_type=f32)
                score_1 = lax.dot_general(key_1, query, rows_by_rows, preferred_element_type=f32)
                dot = lax.dot_general(value, grad, rows_by_rows, preferred_element_type=f32)
                map_0 = jnp.exp2(score_0 * (log2_e / 8) - log_0)
                map_1 = jnp.exp2(score_1 * (log2_e / 8) - log_1)
                if masked:
                    row = lax.broadcasted_iota(jnp.int32, (key_len, 1), 0) + key
                    key_pos = (row // 256 - col) * 512 + half * 256 + row % 256
                    tok_pos = lax.broadcasted_iota(jnp.int32, (1, tok_len), 1) + tok
                    visible = key_pos <= tok_pos
                    map_0 = jnp.where(visible, map_0, 0.0)
                    map_1 = jnp.where(visible, map_1, 0.0)
                grad_0 = (map_0 * (dot - term_0)).astype(bf16)
                grad_1 = (map_1 * (term_1 - dot)).astype(bf16)
                mixed = (map_0 - map_1).astype(bf16)
                dk_ref[group, keys, :] += lax.dot_general(
                    grad_0, query_0, rows_by_cols, preferred_element_type=f32
                ) + lax.dot_general(grad_1, query_1, rows_by_cols, preferred_element_type=f32)
                dv_ref[group, keys, :] += lax.dot_general(
                    mixed, grad, rows_by_cols, preferred_element_type=f32
                )
                dq_ref[block, toks, :] += lax.dot_general(
                    grad_0, key_0, cols_by_cols, preferred_element_type=f32
                ) + lax.dot_general(grad_1, key_1, cols_by_cols, preferred_element_type=f32)

    def one_step(step, carry):
        diagonal = (step == 0) | (step == first_count)
        pl.when(diagonal)(lambda: tile(step, True))
        pl.when(jnp.logical_not(diagonal))(lambda: tile(step, False))
        return carry

    lax.fori_loop(0, 9, one_step, 0)


def attention(place, queries, rows, keys, values):
    vmem = pl.BlockSpec(memory_space=pltpu.VMEM)
    return pl.pallas_call(
        functools.partial(attention_kernel, key_len=512, tok_len=256),
        out_shape=(
            jax.ShapeDtypeStruct((8, 512, 128), f32),
            jax.ShapeDtypeStruct((2, 1024, 128), f32),
            jax.ShapeDtypeStruct((2, 1024, 128), f32),
        ),
        in_specs=[pl.BlockSpec(memory_space=pltpu.SMEM), vmem, vmem, vmem, vmem],
        out_specs=[vmem, vmem, vmem],
        compiler_params=pltpu.CompilerParams(vmem_limit_bytes=60 * 1024 * 1024),
        cost_estimate=pl.CostEstimate(flops=9 * 1024 * 512 * 2048, bytes_accessed=8 << 20, transcendentals=0),
        name="attention",
    )(place, queries, rows, keys, values)


def per_device(queries, key_vectors, latents, w_value, log_sums, out_pair, cotangent, lambdas, out_gain):
    z, x = lax.axis_index("z"), lax.axis_index("x")
    lam = lambdas[0]
    low = jnp.minimum(z, 7 - z)
    half = jnp.where(z < 4, 0, 1)
    mirror = [(i, 7 - i) for i in range(8)]

    out_grad, first_term, second_term = head_cotangent(out_pair, cotangent, lam, out_gain)
    rows = jnp.stack(
        [log_sums[:, 0] * log2_e, log_sums[:, 1] * log2_e - jnp.log2(lam), first_term, second_term]
    )
    query_all, row_all, latent_all, key_all, value_all = gather(
        jnp.concatenate([queries, out_grad], axis=1),
        jnp.concatenate([rows, jnp.zeros_like(rows)]),
        latents,
        w_value.reshape(8, 256, 128),
        key_vectors.reshape(2, 256, 128),
    )
    upper = z >= 4
    place = jnp.stack([low, x, half]).astype(jnp.int32)
    dq, dk, dv = attention(
        place, query_all, row_all, key_all.reshape(2, 1024, 128), value_all.reshape(2, 1024, 128)
    )

    query_grad = lax.psum_scatter(dq, "z", scatter_dimension=0) * 0.125
    both = jnp.concatenate([dk * 0.125, dv], axis=-1).reshape(2, 4, 256, 256)
    own = lax.psum_scatter(both, "x", scatter_dimension=1)
    kept = jnp.where(upper, own[1], own[0])
    given = jnp.where(upper, own[0], own[1])
    came = lax.ppermute(given, "z", mirror)
    whole = jnp.concatenate([jnp.where(upper, came, kept), jnp.where(upper, kept, came)])
    key_grad, value_grad = whole[:, :128], whole[:, 128:]
    partial = lax.dot_general(
        latent_all, value_grad.astype(bf16), (((1,), (0,)), ((), ())), preferred_element_type=f32
    ).reshape(2048, 128)
    weight_grad = lax.psum_scatter(partial, ("z", "x"), scatter_dimension=0, tiled=True)
    return query_grad, key_grad, value_grad, weight_grad


def solution(mesh):
    grid = Mesh(mesh.devices.reshape(8, 4, 4, 2), ("z", "x", "y", "core"))
    sp, tp = ("z", "x"), ("y", "core")
    return jax.shard_map(
        per_device,
        mesh=grid,
        in_specs=(
            P(sp, tp),
            P(sp, tp),
            P(sp, tp),
            P(None, tp),
            P(sp, tp),
            P(sp, tp),
            P(sp, tp),
            P(tp),
            P(),
        ),
        out_specs=(P(sp, tp), P(sp, tp), P(sp, tp), P(sp, tp)),
        check_vma=False,
    )
```

```python
import functools
import math

import jax
import jax.numpy as jnp
import numpy as np
from jax import lax
from jax.experimental import pallas as pl
from jax.experimental.pallas import tpu as pltpu
from jax.sharding import Mesh, PartitionSpec as P

norm_floor = 0.25
log2_e = math.log2(math.e)
f32 = jnp.float32
bf16 = jnp.bfloat16
rows_by_rows = (((1,), (1,)), ((), ()))
rows_by_cols = (((1,), (0,)), ((), ()))
cols_by_cols = (((0,), (0,)), ((), ()))


def head_cotangent(out_pair, cotangent, lam, out_gain):
    first_out = out_pair[:, :128].astype(f32)
    second_out = out_pair[:, 128:].astype(f32)
    merged = first_out - lam * second_out
    inv_norm = lax.rsqrt(jnp.mean(merged * merged, axis=-1, keepdims=True) + norm_floor)
    scaled = cotangent.astype(f32) * out_gain
    inner_dot = jnp.mean(scaled * merged, axis=-1, keepdims=True)
    out_grad = (inv_norm * scaled - merged * (inv_norm * inv_norm * inv_norm) * inner_dot).astype(bf16)
    wide = out_grad.astype(f32)
    return out_grad, jnp.sum(wide * first_out, axis=-1), jnp.sum(wide * second_out, axis=-1)


mesh_ids = pl.DeviceIdType.MESH


class Sender:
    def __init__(self, send_sems, recv_sems):
        self.send_sems, self.recv_sems, self.copies = send_sems, recv_sems, {}

    def start(self, name, source, target, device):
        place = len(self.copies)
        copy = pltpu.make_async_remote_copy(
            src_ref=source,
            dst_ref=target,
            send_sem=self.send_sems.at[place],
            recv_sem=self.recv_sems.at[place],
            device_id=device,
            device_id_type=mesh_ids,
        )
        self.copies[name] = copy
        copy.start()

    def arrived(self, name):
        self.copies[name].wait_recv()

    def finish(self):
        for copy in self.copies.values():
            copy.wait_send()


def greet(devices):
    barrier = pltpu.get_barrier_semaphore()
    for device in devices:
        pl.semaphore_signal(barrier, inc=1, device_id=device, device_id_type=mesh_ids)
    pl.semaphore_wait(barrier, len(devices))


def gather_kernel(
    query_ref, row_ref, latent_ref, weight_ref, key_ref,
    query_all, row_all, latent_all, key_all, value_all,
    value_own, send_sems, recv_sems,
):
    z, x, y, core = (lax.axis_index(name) for name in ("z", "x", "y", "core"))
    up, down = {"z": lax.rem(z + 1, 8)}, {"z": lax.rem(z + 7, 8)}
    mirror = {"z": 7 - z}
    right, left = {"x": lax.rem(x + 1, 4)}, {"x": lax.rem(x + 3, 4)}
    ahead, behind = {"y": lax.rem(y + 1, 4)}, {"y": lax.rem(y + 3, 4)}
    partner = {"core": 1 - core}
    greet([up, down, mirror, right, left, ahead, behind, partner])
    sender = Sender(send_sems, recv_sems)
    start, arrived = sender.start, sender.arrived
    group = jnp.where(z < 4, 0, 1)
    half = group
    halves = (pl.ds(0, 256), pl.ds(256, 256))

    def latent_slot(step, part):
        slot = lax.rem(y + step + 4, 4) * 2 + core
        return latent_all.at[slot, halves[part]]

    def latent_to_partner(step, part):
        start(("pair", step, part), latent_slot(step, part), latent_slot(step, part), partner)

    def query_slot(step, part):
        return query_all.at[lax.rem(z + step + 8, 8), halves[part]]

    def send_query(way, hops, part):
        device, sign = (up, -1) if way == "up" else (down, 1)
        source = query_ref.at[halves[part]] if hops == 0 else query_slot(sign * hops, part)
        start((way, hops, part), source, query_slot(sign * hops, part), device)

    def send_rows(way, hops):
        device, sign = (up, -1) if way == "up" else (down, 1)
        slot = row_all.at[lax.rem(z + sign * hops + 8, 8)]
        start((way, hops, "rows"), row_ref if hops == 0 else slot, slot, device)

    def pass_query(hops, step):
        for way, part in (("up", step), ("down", 1 - step)):
            arrived((way, hops, part))
            if hops < 2 or (hops == 2 and step == 0):
                send_query(way, hops + 1, part)
            if step == 0 and hops < (4 if way == "up" else 3):
                arrived((way, hops, "rows"))
                if hops < (3 if way == "up" else 2):
                    send_rows(way, hops + 1)

    def open_share(name, whole, target):
        start((name, "mirror"), whole.at[1 - half], target.at[group, x], mirror)
        start((name, "own", "right"), whole.at[half], target.at[group, x], right)
        start((name, "own", "left"), whole.at[half], target.at[group, x], left)

    def share_mirrored(name, target):
        arrived((name, "mirror"))
        slot = target.at[1 - group, x]
        start((name, "other", "left"), slot, slot, left)
        start((name, "other", "right"), slot, slot, right)

    def share_far(name, target):
        arrived((name, "own", "right"))
        slot = target.at[group, lax.rem(x + 3, 4)]
        start((name, "own", "far"), slot, slot, right)
        arrived((name, "other", "left"))
        slot = target.at[1 - group, lax.rem(x + 1, 4)]
        start((name, "other", "far"), slot, slot, left)

    def close_share(name):
        arrived((name, "own", "left"))
        arrived((name, "other", "right"))
        arrived((name, "own", "far"))
        arrived((name, "other", "far"))

    own_slot = y * 2 + core
    for way, part, device in (("ahead", 0, ahead), ("behind", 1, behind), ("ahead", 1, ahead), ("behind", 0, behind)):
        start((way, part), latent_ref.at[halves[part]], latent_all.at[own_slot, halves[part]], device)
    start("pair", latent_ref, latent_all.at[own_slot], partner)
    send_query("up", 0, 0)
    send_query("down", 0, 1)
    send_rows("up", 0)
    send_rows("down", 0)
    open_share("key", key_ref, key_all)
    send_query("up", 0, 1)
    send_query("down", 0, 0)
    latent_all[own_slot] = latent_ref[...]
    query_all[z] = query_ref[...]
    row_all[z] = row_ref[...]
    key_all[group, x] = key_ref[half]

    arrived(("ahead", 0))
    start(("ahead", "far"), latent_slot(-1, 0), latent_slot(-1, 0), ahead)
    latent_to_partner(-1, 0)
    arrived(("behind", 1))
    start(("behind", "far"), latent_slot(1, 1), latent_slot(1, 1), behind)
    latent_to_partner(1, 1)
    pass_query(0, 0)
    share_mirrored("key", key_all)
    arrived(("ahead", 1))
    latent_to_partner(-1, 1)
    arrived(("behind", 0))
    latent_to_partner(1, 0)
    pass_query(0, 1)
    share_far("key", key_all)
    arrived(("ahead", "far"))
    latent_to_partner(2, 0)
    arrived(("behind", "far"))
    latent_to_partner(2, 1)
    pass_query(1, 0)
    arrived("pair")
    for step in (-1, 1, 2):
        for part in (0, 1):
            arrived(("pair", step, part))
    total = jnp.zeros((512, 128), f32)
    for slot in range(8):
        total += jnp.dot(latent_all[slot], weight_ref[slot], preferred_element_type=f32)
    own = total.astype(bf16).reshape(2, 256, 128)
    value_own[...] = own
    open_share("value", value_own, value_all)
    value_all[group, x] = value_own[half]
    pass_query(1, 1)
    share_mirrored("value", value_all)
    pass_query(2, 0)
    share_far("value", value_all)
    pass_query(2, 1)
    close_share("key")
    close_share("value")
    pass_query(3, 0)
    sender.finish()


def gather(queries, rows, latents, w_value, keys):
    vmem = pl.BlockSpec(memory_space=pltpu.VMEM)
    return pl.pallas_call(
        gather_kernel,
        out_shape=(
            jax.ShapeDtypeStruct((8, 512, 256), bf16),
            jax.ShapeDtypeStruct((8, 8, 512), f32),
            jax.ShapeDtypeStruct((8, 512, 256), bf16),
            jax.ShapeDtypeStruct((2, 4, 256, 128), bf16),
            jax.ShapeDtypeStruct((2, 4, 256, 128), bf16),
        ),
        in_specs=[vmem] * 5,
        out_specs=[vmem] * 5,
        scratch_shapes=[
            pltpu.VMEM((2, 256, 128), bf16),
            pltpu.SemaphoreType.DMA((48,)),
            pltpu.SemaphoreType.DMA((48,)),
        ],
        compiler_params=pltpu.CompilerParams(
            collective_id=0, has_side_effects=True, vmem_limit_bytes=40 * 1024 * 1024
        ),
        name="gather",
    )(queries, rows, latents, w_value, keys)


def attention_kernel(place, query_ref, row_ref, key_ref, value_ref, dq_out, dk_out, dv_out, dq_ref, dk_ref, dv_ref, *, key_len, tok_len):
    low, col, half = place[0], place[1], place[2]
    dq_ref[...] = jnp.zeros_like(dq_ref)
    dk_ref[...] = jnp.zeros_like(dk_ref)
    dv_ref[...] = jnp.zeros_like(dv_ref)
    first_lanes = lax.broadcasted_iota(jnp.int32, (1, 128), 1) < 64
    first_count = 8 - low

    def split(x):
        zero = jnp.zeros_like(x)
        return jnp.where(first_lanes, x, zero), jnp.where(first_lanes, zero, x)

    def tile(step, masked):
        second = step >= first_count
        group = jnp.where(second, 1, 0)
        block = jnp.where(second, 7 - low + (step - first_count), low + step)
        for tok in range(0, 512, tok_len):
            toks = slice(tok, tok + tok_len)
            query = query_ref[block, toks, 0:128]
            grad = query_ref[block, toks, 128:256]
            query_0, query_1 = split(query)
            log_0, log_1 = row_ref[block, 0:1, toks], row_ref[block, 1:2, toks]
            term_0, term_1 = row_ref[block, 2:3, toks], row_ref[block, 3:4, toks]
            for key in range(0, 1024, key_len):
                keys = slice(key, key + key_len)
                key_0, key_1 = split(key_ref[group, keys, :])
                value = value_ref[group, keys, :]
                score_0 = lax.dot_general(key_0, query, rows_by_rows, preferred_element_type=f32)
                score_1 = lax.dot_general(key_1, query, rows_by_rows, preferred_element_type=f32)
                dot = lax.dot_general(value, grad, rows_by_rows, preferred_element_type=f32)
                map_0 = jnp.exp2(score_0 * (log2_e / 8) - log_0)
                map_1 = jnp.exp2(score_1 * (log2_e / 8) - log_1)
                if masked:
                    row = lax.broadcasted_iota(jnp.int32, (key_len, 1), 0) + key
                    key_pos = (row // 256 - col) * 512 + half * 256 + row % 256
                    tok_pos = lax.broadcasted_iota(jnp.int32, (1, tok_len), 1) + tok
                    visible = key_pos <= tok_pos
                    map_0 = jnp.where(visible, map_0, 0.0)
                    map_1 = jnp.where(visible, map_1, 0.0)
                grad_0 = (map_0 * (dot - term_0)).astype(bf16)
                grad_1 = (map_1 * (term_1 - dot)).astype(bf16)
                mixed = (map_0 - map_1).astype(bf16)
                dk_ref[group, keys, :] += lax.dot_general(
                    grad_0, query_0, rows_by_cols, preferred_element_type=f32
                ) + lax.dot_general(grad_1, query_1, rows_by_cols, preferred_element_type=f32)
                dv_ref[group, keys, :] += lax.dot_general(
                    mixed, grad, rows_by_cols, preferred_element_type=f32
                )
                dq_ref[block, toks, :] += lax.dot_general(
                    grad_0, key_0, cols_by_cols, preferred_element_type=f32
                ) + lax.dot_general(grad_1, key_1, cols_by_cols, preferred_element_type=f32)

    def one_step(step, carry):
        diagonal = (step == 0) | (step == first_count)
        pl.when(diagonal)(lambda: tile(step, True))
        pl.when(jnp.logical_not(diagonal))(lambda: tile(step, False))
        return carry

    lax.fori_loop(0, 9, one_step, 0)
    dq_out[...] = dq_ref[...].astype(bf16)
    dk_out[...] = dk_ref[...].astype(bf16)
    dv_out[...] = dv_ref[...].astype(bf16)


def attention(place, queries, rows, keys, values):
    vmem = pl.BlockSpec(memory_space=pltpu.VMEM)
    return pl.pallas_call(
        functools.partial(attention_kernel, key_len=512, tok_len=256),
        out_shape=(
            jax.ShapeDtypeStruct((8, 512, 128), bf16),
            jax.ShapeDtypeStruct((2, 1024, 128), bf16),
            jax.ShapeDtypeStruct((2, 1024, 128), bf16),
        ),
        in_specs=[pl.BlockSpec(memory_space=pltpu.SMEM), vmem, vmem, vmem, vmem],
        out_specs=[vmem, vmem, vmem],
        scratch_shapes=[
            pltpu.VMEM((8, 512, 128), f32),
            pltpu.VMEM((2, 1024, 128), f32),
            pltpu.VMEM((2, 1024, 128), f32),
        ],
        compiler_params=pltpu.CompilerParams(vmem_limit_bytes=60 * 1024 * 1024),
        cost_estimate=pl.CostEstimate(flops=9 * 1024 * 512 * 2048, bytes_accessed=8 << 20, transcendentals=0),
        name="attention",
    )(place, queries, rows, keys, values)


def scatter_kernel(
    dq_ref, dk_ref, dv_ref, latent_ref, dq_out, dk_out, dv_out, weight_out,
    dq_in, dq_stage, key_in, key_stage, mirror_stage, mirror_in, value_narrow,
    weight_stage, weight_in, weight_pass, weight_mine, weight_last, send_sems, recv_sems,
):
    z, x = lax.axis_index("z"), lax.axis_index("x")
    others = [{"z": lax.rem(z + hops, 8)} for hops in range(1, 8)]
    up, down, mirror = others[0], others[6], {"z": 7 - z}
    right, left = {"x": lax.rem(x + 1, 4)}, {"x": lax.rem(x + 3, 4)}
    greet(others + [right, left])
    sender = Sender(send_sems, recv_sems)
    start, arrived = sender.start, sender.arrived
    group = jnp.where(z < 4, 0, 1)
    rows = (pl.ds(0, 256), pl.ds(256, 256))

    def send_query(way, hops, part):
        number = 0 if way == "up" else 1
        device, sign = (up, 1) if way == "up" else (down, -1)
        source = dq_ref.at[lax.rem(z + sign * hops + 8, 8), rows[part]]
        if not (hops == 4 or (hops == 3 and part != number)):
            arrived((way, hops + 1, part))
            stage = dq_stage.at[number, hops - 1, part]
            stage[...] = (source[...].astype(f32) + dq_in[number, hops, part].astype(f32)).astype(bf16)
            source = stage
        start((way, hops, part), source, dq_in.at[number, hops - 1, part], device)

    def send_column(name, way, hops, part, pieces, inbox, stages):
        number = 0 if way == "right" else 1
        device, sign = (right, 1) if way == "right" else (left, -1)
        source = pieces(lax.rem(x + sign * hops + 4, 4), part)
        if hops == 1 and part == number:
            arrived((name, way, 2, part))
            stage = stages.at[number]
            stage[...] = (source[...].astype(f32) + inbox[number, 2].astype(f32)).astype(bf16)
            source = stage
        slot = 2 if hops == 2 else part
        start((name, way, hops, part), source, inbox.at[number, slot], device)

    def column_sum(name, part, pieces, inbox):
        arrived((name, "right", 1, part))
        arrived((name, "left", 1, part))
        return (
            pieces(x, part)[...].astype(f32) + inbox[0, part].astype(f32) + inbox[1, part].astype(f32)
        )

    def first_columns(name, *args):
        send_column(name, "right", 2, 0, *args)
        send_column(name, "left", 2, 1, *args)
        send_column(name, "right", 1, 1, *args)
        send_column(name, "left", 1, 0, *args)

    def last_columns(name, *args):
        send_column(name, "right", 1, 0, *args)
        send_column(name, "left", 1, 1, *args)

    value_args = (lambda j, part: dv_ref.at[part, j]), key_in.at[0], key_stage.at[0]
    key_args = (lambda j, part: dk_ref.at[part, j]), key_in.at[1], key_stage.at[1]
    weight_args = (lambda j, part: weight_stage.at[j, pl.ds(4 * part, 4)]), weight_in, weight_pass

    def own_rows(name, number, args, out):
        sums = [column_sum(name, part, args[0], args[1]) for part in (0, 1)]
        upper = z >= 4
        mirror_stage[number] = jnp.where(upper, sums[0], sums[1]).astype(bf16)
        out[group] = jnp.where(upper, sums[1], sums[0])
        start((name, "mirror"), mirror_stage.at[number], mirror_in.at[number], mirror)

    first_columns("value", *value_args)
    send_query("up", 4, 0)
    send_query("down", 4, 1)
    send_query("up", 3, 1)
    send_query("down", 3, 0)
    first_columns("key", *key_args)
    last_columns("value", *value_args)
    send_query("up", 3, 0)
    send_query("down", 3, 1)
    own_rows("value", 0, value_args, dv_out)
    last_columns("key", *key_args)
    send_query("up", 2, 1)
    send_query("down", 2, 0)
    value_narrow[group] = dv_out[group].astype(bf16)
    arrived(("value", "mirror"))
    value_narrow[1 - group] = mirror_in[0]
    dv_out[1 - group] = mirror_in[0].astype(f32)
    narrow = value_narrow[...].reshape(512, 128)
    for block in range(8):
        part = lax.dot_general(latent_ref[block], narrow, cols_by_cols, preferred_element_type=f32)
        weight_stage[:, block] = part.astype(bf16).reshape(4, 64, 128)
        if block == 3:
            send_column("weight", "right", 2, 0, *weight_args)
            send_column("weight", "left", 1, 0, *weight_args)
    send_column("weight", "left", 2, 1, *weight_args)
    send_column("weight", "right", 1, 1, *weight_args)
    send_query("up", 2, 0)
    send_query("down", 2, 1)
    send_query("up", 1, 1)
    send_query("down", 1, 0)
    last_columns("weight", *weight_args)
    own_rows("key", 1, key_args, dk_out)
    send_query("up", 1, 0)
    send_query("down", 1, 1)
    for part in (0, 1):
        weight_mine[pl.ds(4 * part, 4)] = column_sum("weight", part, *weight_args[:2]).astype(bf16)
    for hops in range(1, 8):
        start(("weight", hops), weight_mine.at[lax.rem(z + hops, 8)], weight_last.at[hops - 1], others[hops - 1])
    for part in (0, 1):
        arrived(("up", 1, part))
        arrived(("down", 1, part))
        dq_out[rows[part]] = 0.125 * (
            dq_ref[z, rows[part]].astype(f32)
            + dq_in[0, 0, part].astype(f32)
            + dq_in[1, 0, part].astype(f32)
        )
    arrived(("key", "mirror"))
    dk_out[group] = 0.125 * dk_out[group]
    dk_out[1 - group] = 0.125 * mirror_in[1].astype(f32)
    total = weight_mine[z].astype(f32)
    for hops in range(1, 8):
        arrived(("weight", hops))
        total += weight_last[hops - 1].astype(f32)
    weight_out[...] = total
    sender.finish()


def scatter(dq, dk, dv, latents):
    vmem = pl.BlockSpec(memory_space=pltpu.VMEM)
    piece = (256, 128)
    return pl.pallas_call(
        scatter_kernel,
        out_shape=(
            jax.ShapeDtypeStruct((512, 128), f32),
            jax.ShapeDtypeStruct((2, 256, 128), f32),
            jax.ShapeDtypeStruct((2, 256, 128), f32),
            jax.ShapeDtypeStruct((64, 128), f32),
        ),
        in_specs=[vmem] * 4,
        out_specs=[vmem] * 4,
        scratch_shapes=[
            pltpu.VMEM((2, 4, 2, *piece), bf16),
            pltpu.VMEM((2, 3, 2, *piece), bf16),
            pltpu.VMEM((2, 2, 3, *piece), bf16),
            pltpu.VMEM((2, 2, *piece), bf16),
            pltpu.VMEM((2, *piece), bf16),
            pltpu.VMEM((2, *piece), bf16),
            pltpu.VMEM((2, *piece), bf16),
            pltpu.VMEM((4, 8, 64, 128), bf16),
            pltpu.VMEM((2, 3, 4, 64, 128), bf16),
            pltpu.VMEM((2, 4, 64, 128), bf16),
            pltpu.VMEM((8, 64, 128), bf16),
            pltpu.VMEM((7, 64, 128), bf16),
            pltpu.SemaphoreType.DMA((48,)),
            pltpu.SemaphoreType.DMA((48,)),
        ],
        compiler_params=pltpu.CompilerParams(
            collective_id=1, has_side_effects=True, vmem_limit_bytes=40 * 1024 * 1024
        ),
        name="scatter",
    )(dq, dk, dv, latents)


def per_device(queries, key_vectors, latents, w_value, log_sums, out_pair, cotangent, lambdas, out_gain):
    z, x = lax.axis_index("z"), lax.axis_index("x")
    lam = lambdas[0]
    low = jnp.minimum(z, 7 - z)
    half = jnp.where(z < 4, 0, 1)

    out_grad, first_term, second_term = head_cotangent(out_pair, cotangent, lam, out_gain)
    rows = jnp.stack(
        [log_sums[:, 0] * log2_e, log_sums[:, 1] * log2_e - jnp.log2(lam), first_term, second_term]
    )
    query_all, row_all, latent_all, key_all, value_all = gather(
        jnp.concatenate([queries, out_grad], axis=1),
        jnp.concatenate([rows, jnp.zeros_like(rows)]),
        latents,
        w_value.reshape(8, 256, 128),
        key_vectors.reshape(2, 256, 128),
    )
    place = jnp.stack([low, x, half]).astype(jnp.int32)
    dq, dk, dv = attention(
        place, query_all, row_all, key_all.reshape(2, 1024, 128), value_all.reshape(2, 1024, 128)
    )

    query_grad, key_grad, value_grad, weight_grad = scatter(
        dq, dk.reshape(2, 4, 256, 128), dv.reshape(2, 4, 256, 128), latent_all
    )
    return query_grad, key_grad.reshape(512, 128), value_grad.reshape(512, 128), weight_grad


def solution(mesh):
    grid = Mesh(mesh.devices.reshape(8, 4, 4, 2), ("z", "x", "y", "core"))
    sp, tp = ("z", "x"), ("y", "core")
    return jax.shard_map(
        per_device,
        mesh=grid,
        in_specs=(
            P(sp, tp),
            P(sp, tp),
            P(sp, tp),
            P(None, tp),
            P(sp, tp),
            P(sp, tp),
            P(sp, tp),
            P(tp),
            P(),
        ),
        out_specs=(P(sp, tp), P(sp, tp), P(sp, tp), P(sp, tp)),
        check_vma=False,
    )
```

```python
import functools
import math

import jax
import jax.numpy as jnp
from jax import lax
from jax.experimental import pallas as pl
from jax.experimental.pallas import tpu as pltpu
from jax.sharding import Mesh, PartitionSpec as P

norm_floor = 0.25
log2_e = math.log2(math.e)
f32 = jnp.float32
bf16 = jnp.bfloat16
rows_by_rows = (((1,), (1,)), ((), ()))
rows_by_cols = (((1,), (0,)), ((), ()))
cols_by_cols = (((0,), (0,)), ((), ()))
mesh_ids = pl.DeviceIdType.MESH
key_len, tok_len = 512, 256


class Sender:
    def __init__(self, send_sems, recv_sems):
        self.send_sems, self.recv_sems, self.copies = send_sems, recv_sems, {}

    def start(self, name, source, target, device):
        place = len(self.copies)
        copy = pltpu.make_async_remote_copy(
            src_ref=source,
            dst_ref=target,
            send_sem=self.send_sems.at[place],
            recv_sem=self.recv_sems.at[place],
            device_id=device,
            device_id_type=mesh_ids,
        )
        self.copies[name] = copy
        copy.start()

    def arrived(self, name):
        self.copies[name].wait_recv()

    def finish(self):
        for copy in self.copies.values():
            copy.wait_send()


def greet(devices):
    barrier = pltpu.get_barrier_semaphore()
    for device in devices:
        pl.semaphore_signal(barrier, inc=1, device_id=device, device_id_type=mesh_ids)
    pl.semaphore_wait(barrier, len(devices))


def turned(index, step, size):
    return lax.rem(index + (step + size), size)


def whole_kernel(
    query_hbm, key_hbm, latent_hbm, weight_hbm, log_hbm, pair_hbm, cotangent_hbm, gain_hbm, lam_ref,
    dq_out, dk_out, dv_out, weight_out,
    query_all, row_all, latent_all, key_all, value_all,
    key_given, weight_ref, log_ref, pair_ref, cotangent_ref, gain_ref, value_own,
    dq_acc, dk_acc, dv_acc, dq_in, dq_stage, column_in, column_stage,
    mirror_stage, mirror_in, value_narrow,
    weight_part, weight_stage, weight_in, weight_mine, weight_last,
    local_sems, send_sems, recv_sems,
):
    z, x, y, core = (lax.axis_index(name) for name in ("z", "x", "y", "core"))
    group = jnp.where(z < 4, 0, 1)
    half = group
    own_slot = y * 2 + core

    loads = {}
    for place, (name, source, target) in enumerate(
        (
            ("latent", latent_hbm, latent_all.at[own_slot]),
            ("key", key_hbm.at[half], key_all.at[group, x]),
            ("given", key_hbm.at[1 - half], key_given),
            ("pair", pair_hbm, pair_ref),
            ("cotangent", cotangent_hbm, cotangent_ref),
            ("gain", gain_hbm, gain_ref),
            ("log", log_hbm, log_ref),
            ("query", query_hbm, query_all.at[z, :, pl.ds(0, 128)]),
            ("weight", weight_hbm, weight_ref),
        )
    ):
        loads[name] = pltpu.make_async_copy(source, target, local_sems.at[place])
        loads[name].start()

    others = [{"z": turned(z, hops, 8)} for hops in range(1, 8)]
    up, down, mirror = others[0], others[6], {"z": 7 - z}
    right, left = {"x": turned(x, 1, 4)}, {"x": turned(x, -1, 4)}
    ahead, behind = {"y": turned(y, 1, 4)}, {"y": turned(y, -1, 4)}
    partner = {"core": 1 - core}
    greet(others + [right, left, ahead, behind, partner])
    sender = Sender(send_sems, recv_sems)
    start, arrived = sender.start, sender.arrived
    halves = (pl.ds(0, 256), pl.ds(256, 256))

    def latent_slot(step, part):
        return latent_all.at[turned(y, step, 4) * 2 + core, halves[part]]

    def latent_to_partner(step, part):
        start(("pair", step, part), latent_slot(step, part), latent_slot(step, part), partner)

    def send_query(way, hops, part):
        device, sign = (up, -1) if way == "up" else (down, 1)
        slot = query_all.at[turned(z, sign * hops, 8), halves[part]]
        start((way, hops, part), slot, slot, device)

    def send_rows(way, hops):
        device, sign = (up, -1) if way == "up" else (down, 1)
        slot = row_all.at[turned(z, sign * hops, 8)]
        start((way, hops, "rows"), slot, slot, device)

    def pass_query(hops, step):
        for way, part in (("up", step), ("down", 1 - step)):
            arrived((way, hops, part))
            if hops < 2 or (hops == 2 and step == 0):
                send_query(way, hops + 1, part)
            if step == 0 and hops < (4 if way == "up" else 3):
                arrived((way, hops, "rows"))
                if hops < (3 if way == "up" else 2):
                    send_rows(way, hops + 1)

    def open_share(name, given, target):
        slot = target.at[group, x]
        start((name, "mirror"), given, slot, mirror)
        start((name, "own", "right"), slot, slot, right)
        start((name, "own", "left"), slot, slot, left)

    def share_mirrored(name, target):
        arrived((name, "mirror"))
        slot = target.at[1 - group, x]
        start((name, "other", "left"), slot, slot, left)
        start((name, "other", "right"), slot, slot, right)

    def share_far(name, target):
        arrived((name, "own", "right"))
        slot = target.at[group, turned(x, -1, 4)]
        start((name, "own", "far"), slot, slot, right)
        arrived((name, "other", "left"))
        slot = target.at[1 - group, turned(x, 1, 4)]
        start((name, "other", "far"), slot, slot, left)

    def close_share(name):
        arrived((name, "own", "left"))
        arrived((name, "other", "right"))
        arrived((name, "own", "far"))
        arrived((name, "other", "far"))

    loads["latent"].wait()
    for way, part, device in (("ahead", 0, ahead), ("behind", 1, behind), ("ahead", 1, ahead), ("behind", 0, behind)):
        slot = latent_all.at[own_slot, halves[part]]
        start((way, part), slot, slot, device)
    start("pair", latent_all.at[own_slot], latent_all.at[own_slot], partner)
    loads["key"].wait()
    loads["given"].wait()
    open_share("key", key_given, key_all)

    for name in ("pair", "cotangent", "gain", "log", "query"):
        loads[name].wait()
    lam = lam_ref[0]
    first_out, second_out = pair_ref[:, 0:128].astype(f32), pair_ref[:, 128:256].astype(f32)
    merged = first_out - lam * second_out
    inv_norm = lax.rsqrt(jnp.mean(merged * merged, axis=-1, keepdims=True) + norm_floor)
    scaled = cotangent_ref[...].astype(f32) * gain_ref[...]
    inner_dot = jnp.mean(scaled * merged, axis=-1, keepdims=True)
    out_grad = (inv_norm * scaled - merged * (inv_norm * inv_norm * inv_norm) * inner_dot).astype(bf16)
    query_all[z, :, 128:256] = out_grad
    wide = out_grad.astype(f32)
    first_term = jnp.sum(wide * first_out, axis=-1, keepdims=True)
    second_term = jnp.sum(wide * second_out, axis=-1, keepdims=True)
    lane = lax.broadcasted_iota(jnp.int32, (1, 128), 1)
    terms = jnp.where(lane == 2, first_term, jnp.where(lane == 3, second_term, 0.0)).T[0:8]
    log_lam = jnp.log(jnp.full((1, 512), lam, f32)) * log2_e
    row_all[z] = terms
    row_all[z, 0:1, :] = log_ref[0:1, :] * log2_e
    row_all[z, 1:2, :] = log_ref[1:2, :] * log2_e - log_lam
    send_query("up", 0, 0)
    send_query("down", 0, 1)
    send_rows("up", 0)
    send_rows("down", 0)
    send_query("up", 0, 1)
    send_query("down", 0, 0)

    dq_acc[...] = jnp.zeros_like(dq_acc)
    dk_acc[...] = jnp.zeros_like(dk_acc)
    dv_acc[...] = jnp.zeros_like(dv_acc)

    arrived(("ahead", 0))
    start(("ahead", "far"), latent_slot(-1, 0), latent_slot(-1, 0), ahead)
    latent_to_partner(-1, 0)
    arrived(("behind", 1))
    start(("behind", "far"), latent_slot(1, 1), latent_slot(1, 1), behind)
    latent_to_partner(1, 1)
    share_mirrored("key", key_all)
    pass_query(0, 0)
    arrived(("ahead", 1))
    latent_to_partner(-1, 1)
    arrived(("behind", 0))
    latent_to_partner(1, 0)
    share_far("key", key_all)
    pass_query(0, 1)
    arrived(("ahead", "far"))
    latent_to_partner(2, 0)
    arrived(("behind", "far"))
    latent_to_partner(2, 1)
    arrived("pair")
    for step in (-1, 1, 2):
        for part in (0, 1):
            arrived(("pair", step, part))
    loads["weight"].wait()
    total = jnp.zeros((512, 128), f32)
    for slot in range(8):
        total += jnp.dot(latent_all[slot], weight_ref[slot], preferred_element_type=f32)
    value_own[...] = total.astype(bf16).reshape(2, 256, 128)
    value_all[group, x] = value_own[half]
    open_share("value", value_own.at[1 - half], value_all)
    pass_query(1, 0)
    share_mirrored("value", value_all)
    pass_query(1, 1)
    share_far("value", value_all)
    pass_query(2, 0)
    close_share("key")
    close_share("value")
    pass_query(2, 1)
    pass_query(3, 0)

    first_lanes = lane < 64

    def split(value):
        zero = jnp.zeros_like(value)
        return jnp.where(first_lanes, value, zero), jnp.where(first_lanes, zero, value)

    def tile(part, block, masked):
        for tok in range(0, 512, tok_len):
            toks = slice(tok, tok + tok_len)
            query, grad = query_all[block, toks, 0:128], query_all[block, toks, 128:256]
            query_0, query_1 = split(query)
            log_0, log_1 = row_all[block, 0:1, toks], row_all[block, 1:2, toks]
            term_0, term_1 = row_all[block, 2:3, toks], row_all[block, 3:4, toks]
            for key in range(0, 1024, key_len):
                cols = slice(key // 256, (key + key_len) // 256)
                key_0, key_1 = split(key_all[part, cols].reshape(key_len, 128))
                value = value_all[part, cols].reshape(key_len, 128)
                score_0 = lax.dot_general(key_0, query, rows_by_rows, preferred_element_type=f32)
                score_1 = lax.dot_general(key_1, query, rows_by_rows, preferred_element_type=f32)
                dot = lax.dot_general(value, grad, rows_by_rows, preferred_element_type=f32)
                map_0 = jnp.exp2(score_0 * (log2_e / 8) - log_0)
                map_1 = jnp.exp2(score_1 * (log2_e / 8) - log_1)
                if masked:
                    row = lax.broadcasted_iota(jnp.int32, (key_len, 1), 0) + key
                    key_pos = (row // 256 - x) * 512 + half * 256 + row % 256
                    tok_pos = lax.broadcasted_iota(jnp.int32, (1, tok_len), 1) + tok
                    visible = key_pos <= tok_pos
                    map_0 = jnp.where(visible, map_0, 0.0)
                    map_1 = jnp.where(visible, map_1, 0.0)
                grad_0 = (map_0 * (dot - term_0)).astype(bf16)
                grad_1 = (map_1 * (term_1 - dot)).astype(bf16)
                mixed = (map_0 - map_1).astype(bf16)
                dk = lax.dot_general(
                    grad_0, query_0, rows_by_cols, preferred_element_type=f32
                ) + lax.dot_general(grad_1, query_1, rows_by_cols, preferred_element_type=f32)
                dv = lax.dot_general(mixed, grad, rows_by_cols, preferred_element_type=f32)
                dk_acc[part, cols] += dk.reshape(key_len // 256, 256, 128)
                dv_acc[part, cols] += dv.reshape(key_len // 256, 256, 128)
                dq_acc[block, toks, :] += lax.dot_general(
                    grad_0, key_0, cols_by_cols, preferred_element_type=f32
                ) + lax.dot_general(grad_1, key_1, cols_by_cols, preferred_element_type=f32)

    def tiles(part, begin):
        def one(block, carry):
            tile(part, block, False)
            return carry

        lax.fori_loop(begin, 8, one, 0)

    def send_column(name, way, hops, part, pieces, inbox, stages):
        number = 0 if way == "right" else 1
        device, sign = (right, 1) if way == "right" else (left, -1)
        value = pieces(turned(x, sign * hops, 4), part)
        place = 0 if hops == 2 else 1
        if hops == 1 and part == number:
            arrived((name, way, 2, part))
            value += inbox[number, 2].astype(f32)
            place = 2
        stages[number, place] = value.astype(bf16)
        slot = 2 if hops == 2 else part
        start((name, way, hops, part), stages.at[number, place], inbox.at[number, slot], device)

    def first_columns(name, *args):
        send_column(name, "right", 2, 0, *args)
        send_column(name, "left", 2, 1, *args)
        send_column(name, "right", 1, 1, *args)
        send_column(name, "left", 1, 0, *args)

    def last_columns(name, *args):
        send_column(name, "right", 1, 0, *args)
        send_column(name, "left", 1, 1, *args)

    def column_sum(name, part, pieces, inbox):
        arrived((name, "right", 1, part))
        arrived((name, "left", 1, part))
        return pieces(x, part) + inbox[0, part].astype(f32) + inbox[1, part].astype(f32)

    def sum_args(acc, rows_of, number):
        def pieces(j, part):
            return acc[rows_of, j, 128 * part : 128 * part + 128, :]

        return pieces, column_in.at[number], column_stage.at[number]

    other_value, other_key = sum_args(dv_acc, 1 - group, 0), sum_args(dk_acc, 1 - group, 1)
    own_value, own_key = sum_args(dv_acc, group, 2), sum_args(dk_acc, group, 3)

    def mirrored_rows(name, number, args):
        for part in (0, 1):
            mirror_stage[number, 128 * part : 128 * part + 128] = column_sum(name, part, *args[:2]).astype(bf16)
        start((name, "mirror back"), mirror_stage.at[number], mirror_in.at[number], mirror)

    def own_rows(name, args, out):
        for part in (0, 1):
            out[group, 128 * part : 128 * part + 128] = column_sum(name, part, *args[:2])

    def send_dq(way, hops, part):
        number = 0 if way == "up" else 1
        device, sign = (up, 1) if way == "up" else (down, -1)
        value = dq_acc[turned(z, sign * hops, 8), halves[part]]
        if not (hops == 4 or (hops == 3 and part != number)):
            arrived(("dq", way, hops + 1, part))
            value += dq_in[number, hops, part].astype(f32)
        dq_stage[number, hops - 1, part] = value.astype(bf16)
        start(
            ("dq", way, hops, part),
            dq_stage.at[number, hops - 1, part],
            dq_in.at[number, hops - 1, part],
            device,
        )

    tile(1 - group, 7 - z, True)
    tiles(1 - group, 8 - z)
    first_columns("other value", *other_value)
    first_columns("other key", *other_key)
    tile(group, z, True)
    last_columns("other value", *other_value)
    last_columns("other key", *other_key)
    tiles(group, z + 1)
    first_columns("own value", *own_value)
    mirrored_rows("other value", 0, other_value)
    send_dq("up", 4, 0)
    send_dq("down", 4, 1)
    send_dq("up", 3, 1)
    send_dq("down", 3, 0)
    last_columns("own value", *own_value)
    first_columns("own key", *own_key)
    mirrored_rows("other key", 1, other_key)
    own_rows("own value", own_value, dv_out)
    value_narrow[group] = dv_out[group].astype(bf16)
    send_dq("up", 3, 0)
    send_dq("down", 3, 1)
    last_columns("own key", *own_key)
    arrived(("other value", "mirror back"))
    value_narrow[1 - group] = mirror_in[0]
    dv_out[1 - group] = mirror_in[0].astype(f32)

    weight_args = (lambda j, part: weight_part[j, 4 * part : 4 * part + 4]), weight_in, weight_stage
    narrow = value_narrow[...].reshape(512, 128)
    for block in range(8):
        part = lax.dot_general(latent_all[block], narrow, cols_by_cols, preferred_element_type=f32)
        weight_part[:, block] = part.reshape(4, 64, 128)
        if block == 3:
            send_column("weight", "right", 2, 0, *weight_args)
            send_column("weight", "left", 1, 0, *weight_args)
    send_column("weight", "left", 2, 1, *weight_args)
    send_column("weight", "right", 1, 1, *weight_args)
    send_dq("up", 2, 1)
    send_dq("down", 2, 0)
    own_rows("own key", own_key, dk_out)
    send_dq("up", 2, 0)
    send_dq("down", 2, 1)
    last_columns("weight", *weight_args)
    send_dq("up", 1, 1)
    send_dq("down", 1, 0)
    for part in (0, 1):
        weight_mine[4 * part : 4 * part + 4] = column_sum("weight", part, *weight_args[:2]).astype(bf16)
    for hops in range(1, 8):
        start(("weight", hops), weight_mine.at[turned(z, hops, 8)], weight_last.at[hops - 1], others[hops - 1])
    send_dq("up", 1, 0)
    send_dq("down", 1, 1)
    arrived(("other key", "mirror back"))
    dk_out[group] = 0.125 * dk_out[group]
    dk_out[1 - group] = 0.125 * mirror_in[1].astype(f32)
    for part in (0, 1):
        arrived(("dq", "up", 1, part))
        arrived(("dq", "down", 1, part))
        dq_out[halves[part]] = 0.125 * (
            dq_acc[z, halves[part]] + dq_in[0, 0, part].astype(f32) + dq_in[1, 0, part].astype(f32)
        )
    total = weight_mine[z].astype(f32)
    for hops in range(1, 8):
        arrived(("weight", hops))
        total += weight_last[hops - 1].astype(f32)
    weight_out[...] = total
    sender.finish()


def per_device(queries, key_vectors, latents, w_value, log_sums, out_pair, cotangent, lambdas, out_gain):
    anywhere, vmem = pl.BlockSpec(memory_space=pl.ANY), pl.BlockSpec(memory_space=pltpu.VMEM)
    scratch = (
        ((8, 512, 256), bf16),
        ((8, 8, 512), f32),
        ((8, 512, 256), bf16),
        ((2, 4, 256, 128), bf16),
        ((2, 4, 256, 128), bf16),
        ((256, 128), bf16),
        ((8, 256, 128), bf16),
        ((2, 512), f32),
        ((512, 256), bf16),
        ((512, 128), bf16),
        ((1, 128), f32),
        ((2, 256, 128), bf16),
        ((8, 512, 128), f32),
        ((2, 4, 256, 128), f32),
        ((2, 4, 256, 128), f32),
        ((2, 4, 2, 256, 128), bf16),
        ((2, 4, 2, 256, 128), bf16),
        ((4, 2, 3, 128, 128), bf16),
        ((4, 2, 3, 128, 128), bf16),
        ((2, 256, 128), bf16),
        ((2, 256, 128), bf16),
        ((2, 256, 128), bf16),
        ((4, 8, 64, 128), f32),
        ((2, 3, 4, 64, 128), bf16),
        ((2, 3, 4, 64, 128), bf16),
        ((8, 64, 128), bf16),
        ((7, 64, 128), bf16),
    )
    query_grad, key_grad, value_grad, weight_grad = pl.pallas_call(
        whole_kernel,
        out_shape=(
            jax.ShapeDtypeStruct((512, 128), f32),
            jax.ShapeDtypeStruct((2, 256, 128), f32),
            jax.ShapeDtypeStruct((2, 256, 128), f32),
            jax.ShapeDtypeStruct((64, 128), f32),
        ),
        in_specs=[anywhere] * 8 + [pl.BlockSpec(memory_space=pltpu.SMEM)],
        out_specs=[vmem] * 4,
        scratch_shapes=[pltpu.VMEM(*entry) for entry in scratch]
        + [
            pltpu.SemaphoreType.DMA((9,)),
            pltpu.SemaphoreType.DMA((110,)),
            pltpu.SemaphoreType.DMA((110,)),
        ],
        compiler_params=pltpu.CompilerParams(
            collective_id=0, has_side_effects=True, vmem_limit_bytes=60 * 1024 * 1024
        ),
        name="whole",
    )(
        queries,
        key_vectors.reshape(2, 256, 128),
        latents,
        w_value.reshape(8, 256, 128),
        log_sums.T,
        out_pair,
        cotangent,
        out_gain.reshape(1, 128),
        lambdas,
    )
    return query_grad, key_grad.reshape(512, 128), value_grad.reshape(512, 128), weight_grad


def solution(mesh):
    grid = Mesh(mesh.devices.reshape(8, 4, 4, 2), ("z", "x", "y", "core"))
    sp, tp = ("z", "x"), ("y", "core")
    return jax.shard_map(
        per_device,
        mesh=grid,
        in_specs=(
            P(sp, tp),
            P(sp, tp),
            P(sp, tp),
            P(None, tp),
            P(sp, tp),
            P(sp, tp),
            P(sp, tp),
            P(tp),
            P(),
        ),
        out_specs=(P(sp, tp), P(sp, tp), P(sp, tp), P(sp, tp)),
        check_vma=False,
    )
```

```python
import functools
import math

import jax
import jax.numpy as jnp
from jax import lax
from jax.experimental import pallas as pl
from jax.experimental.pallas import tpu as pltpu
from jax.sharding import Mesh, PartitionSpec as P

norm_floor = 0.25
log2_e = math.log2(math.e)
f32 = jnp.float32
bf16 = jnp.bfloat16
rows_by_rows = (((1,), (1,)), ((), ()))
rows_by_cols = (((1,), (0,)), ((), ()))
cols_by_cols = (((0,), (0,)), ((), ()))
mesh_ids = pl.DeviceIdType.MESH
key_len, tok_len = 1024, 256


class Sender:
    def __init__(self, send_sems, recv_sems):
        self.send_sems, self.recv_sems, self.copies = send_sems, recv_sems, {}

    def start(self, name, source, target, device):
        place = len(self.copies)
        copy = pltpu.make_async_remote_copy(
            src_ref=source,
            dst_ref=target,
            send_sem=self.send_sems.at[place],
            recv_sem=self.recv_sems.at[place],
            device_id=device,
            device_id_type=mesh_ids,
        )
        self.copies[name] = copy
        copy.start()

    def arrived(self, name):
        self.copies[name].wait_recv()

    def finish(self):
        for copy in self.copies.values():
            copy.wait_send()


def greet(devices):
    barrier = pltpu.get_barrier_semaphore()
    for device in devices:
        pl.semaphore_signal(barrier, inc=1, device_id=device, device_id_type=mesh_ids)
    pl.semaphore_wait(barrier, len(devices))


def turned(index, step, size):
    return lax.rem(index + (step + size), size)


def whole_kernel(
    query_hbm, key_hbm, latent_hbm, weight_hbm, log_hbm, pair_hbm, cotangent_hbm, gain_hbm, lam_ref,
    dq_out, dk_out, dv_out, weight_out,
    query_all, row_all, latent_all, key_all, value_all,
    key_given, weight_ref, log_ref, pair_ref, cotangent_ref, gain_ref, value_own,
    dq_acc, dk_acc, dv_acc, dq_in, dq_stage, column_in, column_stage,
    mirror_stage, mirror_in, value_narrow,
    weight_part, weight_stage, weight_in, weight_mine, weight_last,
    local_sems, send_sems, recv_sems,
):
    z, x, y, core = (lax.axis_index(name) for name in ("z", "x", "y", "core"))
    group = jnp.where(z < 4, 0, 1)
    half = group
    own_slot = y * 2 + core

    loads = {}
    for place, (name, source, target) in enumerate(
        (
            ("latent", latent_hbm, latent_all.at[own_slot]),
            ("key", key_hbm.at[half], key_all.at[group, x]),
            ("given", key_hbm.at[1 - half], key_given),
            ("pair", pair_hbm, pair_ref),
            ("cotangent", cotangent_hbm, cotangent_ref),
            ("gain", gain_hbm, gain_ref),
            ("log", log_hbm, log_ref),
            ("query", query_hbm, query_all.at[z, :, pl.ds(0, 128)]),
            ("weight", weight_hbm, weight_ref),
        )
    ):
        loads[name] = pltpu.make_async_copy(source, target, local_sems.at[place])
        loads[name].start()

    others = [{"z": turned(z, hops, 8)} for hops in range(1, 8)]
    up, down, mirror = others[0], others[6], {"z": 7 - z}
    right, left = {"x": turned(x, 1, 4)}, {"x": turned(x, -1, 4)}
    ahead, behind = {"y": turned(y, 1, 4)}, {"y": turned(y, -1, 4)}
    partner = {"core": 1 - core}
    greet(others + [right, left, ahead, behind, partner])
    sender = Sender(send_sems, recv_sems)
    start, arrived = sender.start, sender.arrived
    halves = (pl.ds(0, 256), pl.ds(256, 256))

    def latent_slot(step, toks, part=None):
        slot = latent_all.at[turned(y, step, 4) * 2 + core, toks]
        return slot if part is None else slot.at[:, pl.ds(128 * part, 128)]

    def latent_to_partner(name, step, toks):
        start(("pair", name, step), latent_slot(step, toks), latent_slot(step, toks), partner)

    def open_latents(name, toks):
        for way, part, device in (("ahead", 0, ahead), ("behind", 1, behind), ("ahead", 1, ahead), ("behind", 0, behind)):
            slot = latent_slot(0, toks, part)
            start((name, way, part), slot, slot, device)
        latent_to_partner(name, 0, toks)

    def latents_far(name, toks):
        for way, step, part, device in (("ahead", -1, 0, ahead), ("behind", 1, 1, behind)):
            arrived((name, way, part))
            slot = latent_slot(step, toks, part)
            start((name, way, "far"), slot, slot, device)

    def latents_near(name, toks):
        for way, step, part in (("ahead", -1, 1), ("behind", 1, 0)):
            arrived((name, way, part))
            latent_to_partner(name, step, toks)

    def latents_last(name, toks):
        arrived((name, "ahead", "far"))
        arrived((name, "behind", "far"))
        latent_to_partner(name, 2, toks)

    def values_of(name, toks):
        for step in (0, -1, 1, 2):
            arrived(("pair", name, step))
        total = jnp.zeros((256, 128), f32)
        for slot in range(8):
            total += jnp.dot(latent_all[slot, toks], weight_ref[slot], preferred_element_type=f32)
        return total.astype(bf16)

    def send_query(way, hops, part):
        device, sign = (up, -1) if way == "up" else (down, 1)
        slot = query_all.at[turned(z, sign * hops, 8), halves[part]]
        start((way, hops, part), slot, slot, device)

    def send_rows(way, hops):
        device, sign = (up, -1) if way == "up" else (down, 1)
        slot = row_all.at[turned(z, sign * hops, 8)]
        start((way, hops, "rows"), slot, slot, device)

    def pass_query(hops, step):
        for way, part in (("up", step), ("down", 1 - step)):
            arrived((way, hops, part))
            if hops < 2 or (hops == 2 and step == 0):
                send_query(way, hops + 1, part)
            if step == 0 and hops < (4 if way == "up" else 3):
                arrived((way, hops, "rows"))
                if hops < (3 if way == "up" else 2):
                    send_rows(way, hops + 1)

    def open_share(name, given, target):
        slot = target.at[group, x]
        if given is not None:
            start((name, "mirror"), given, slot, mirror)
        start((name, "own", "right"), slot, slot, right)
        start((name, "own", "left"), slot, slot, left)

    def share_mirrored(name, target):
        arrived((name, "mirror"))
        slot = target.at[1 - group, x]
        start((name, "other", "left"), slot, slot, left)
        start((name, "other", "right"), slot, slot, right)

    def share_far(name, target):
        arrived((name, "own", "right"))
        slot = target.at[group, turned(x, -1, 4)]
        start((name, "own", "far"), slot, slot, right)
        arrived((name, "other", "left"))
        slot = target.at[1 - group, turned(x, 1, 4)]
        start((name, "other", "far"), slot, slot, left)

    def close_share(name):
        arrived((name, "own", "left"))
        arrived((name, "other", "right"))
        arrived((name, "own", "far"))
        arrived((name, "other", "far"))

    loads["latent"].wait()
    open_latents("given", 1 - half)
    loads["key"].wait()
    loads["given"].wait()
    open_share("key", key_given, key_all)

    for name in ("pair", "cotangent", "gain", "log", "query"):
        loads[name].wait()
    lam = lam_ref[0]
    first_out, second_out = pair_ref[:, 0:128].astype(f32), pair_ref[:, 128:256].astype(f32)
    merged = first_out - lam * second_out
    inv_norm = lax.rsqrt(jnp.mean(merged * merged, axis=-1, keepdims=True) + norm_floor)
    scaled = cotangent_ref[...].astype(f32) * gain_ref[...]
    inner_dot = jnp.mean(scaled * merged, axis=-1, keepdims=True)
    out_grad = (inv_norm * scaled - merged * (inv_norm * inv_norm * inv_norm) * inner_dot).astype(bf16)
    query_all[z, :, 128:256] = out_grad
    wide = out_grad.astype(f32)
    first_term = jnp.sum(wide * first_out, axis=-1, keepdims=True)
    second_term = jnp.sum(wide * second_out, axis=-1, keepdims=True)
    lane = lax.broadcasted_iota(jnp.int32, (1, 128), 1)
    terms = jnp.where(lane == 2, first_term, jnp.where(lane == 3, second_term, 0.0)).T[0:8]
    log_lam = jnp.log(jnp.full((1, 512), lam, f32)) * log2_e
    row_all[z] = terms
    row_all[z, 0:1, :] = log_ref[0:1, :] * log2_e
    row_all[z, 1:2, :] = log_ref[1:2, :] * log2_e - log_lam
    send_query("up", 0, 0)
    send_query("down", 0, 1)
    send_rows("up", 0)
    send_rows("down", 0)
    send_query("up", 0, 1)
    send_query("down", 0, 0)

    dq_acc[...] = jnp.zeros_like(dq_acc)
    dk_acc[...] = jnp.zeros_like(dk_acc)
    dv_acc[...] = jnp.zeros_like(dv_acc)

    latents_far("given", 1 - half)
    open_latents("own", half)
    share_mirrored("key", key_all)
    latents_near("given", 1 - half)
    latents_last("given", 1 - half)
    loads["weight"].wait()
    pass_query(0, 0)
    value_own[...] = values_of("given", 1 - half)
    start(("value", "mirror"), value_own, value_all.at[group, x], mirror)
    latents_far("own", half)
    share_far("key", key_all)
    latents_near("own", half)
    pass_query(0, 1)
    latents_last("own", half)
    value_all[group, x] = values_of("own", half)
    open_share("value", None, value_all)
    pass_query(1, 0)
    share_mirrored("value", value_all)
    pass_query(1, 1)
    share_far("value", value_all)
    pass_query(2, 0)
    close_share("key")
    close_share("value")
    pass_query(2, 1)

    first_lanes = lane < 64

    def split(value):
        zero = jnp.zeros_like(value)
        return jnp.where(first_lanes, value, zero), jnp.where(first_lanes, zero, value)

    def tile(part, block, masked):
        for tok in range(0, 512, tok_len):
            toks = slice(tok, tok + tok_len)
            query, grad = query_all[block, toks, 0:128], query_all[block, toks, 128:256]
            query_0, query_1 = split(query)
            dq = jnp.zeros((128, tok_len), f32)
            log_0, log_1 = row_all[block, 0:1, toks], row_all[block, 1:2, toks]
            term_0, term_1 = row_all[block, 2:3, toks], row_all[block, 3:4, toks]
            for key in range(0, 1024, key_len):
                cols = slice(key // 256, (key + key_len) // 256)
                key_0, key_1 = split(key_all[part, cols].reshape(key_len, 128))
                value = value_all[part, cols].reshape(key_len, 128)
                score_0 = lax.dot_general(key_0, query, rows_by_rows, preferred_element_type=f32)
                score_1 = lax.dot_general(key_1, query, rows_by_rows, preferred_element_type=f32)
                dot = lax.dot_general(value, grad, rows_by_rows, preferred_element_type=f32)
                map_0 = jnp.exp2(score_0 * (log2_e / 8) - log_0)
                map_1 = jnp.exp2(score_1 * (log2_e / 8) - log_1)
                if masked:
                    row = lax.broadcasted_iota(jnp.int32, (key_len, 1), 0) + key
                    key_pos = (row // 256 - x) * 512 + half * 256 + row % 256
                    tok_pos = lax.broadcasted_iota(jnp.int32, (1, tok_len), 1) + tok
                    visible = key_pos <= tok_pos
                    map_0 = jnp.where(visible, map_0, 0.0)
                    map_1 = jnp.where(visible, map_1, 0.0)
                grad_0 = (map_0 * (dot - term_0)).astype(bf16)
                grad_1 = (map_1 * (term_1 - dot)).astype(bf16)
                mixed = (map_0 - map_1).astype(bf16)
                dk = lax.dot_general(
                    grad_0, query_0, rows_by_cols, preferred_element_type=f32
                ) + lax.dot_general(grad_1, query_1, rows_by_cols, preferred_element_type=f32)
                dv = lax.dot_general(mixed, grad, rows_by_cols, preferred_element_type=f32)
                dk_acc[part, cols] += dk.reshape(key_len // 256, 256, 128)
                dv_acc[part, cols] += dv.reshape(key_len // 256, 256, 128)
                dq += lax.dot_general(
                    key_0, grad_0, cols_by_cols, preferred_element_type=f32
                ) + lax.dot_general(key_1, grad_1, cols_by_cols, preferred_element_type=f32)
            dq_acc[block, toks, :] += dq.T

    def tiles(part, begin):
        def one(block, carry):
            tile(part, block, False)
            return carry

        lax.fori_loop(begin, 8, one, 0)

    def send_column(name, way, hops, part, pieces, inbox, stages):
        number = 0 if way == "right" else 1
        device, sign = (right, 1) if way == "right" else (left, -1)
        value = pieces(turned(x, sign * hops, 4), part)
        place = 0 if hops == 2 else 1
        if hops == 1 and part == number:
            arrived((name, way, 2, part))
            value += inbox[number, 2].astype(f32)
            place = 2
        stages[number, place] = value.astype(bf16)
        slot = 2 if hops == 2 else part
        start((name, way, hops, part), stages.at[number, place], inbox.at[number, slot], device)

    def first_columns(name, *args):
        send_column(name, "right", 2, 0, *args)
        send_column(name, "left", 2, 1, *args)
        send_column(name, "right", 1, 1, *args)
        send_column(name, "left", 1, 0, *args)

    def last_columns(name, *args):
        send_column(name, "right", 1, 0, *args)
        send_column(name, "left", 1, 1, *args)

    def column_sum(name, part, pieces, inbox):
        arrived((name, "right", 1, part))
        arrived((name, "left", 1, part))
        return pieces(x, part) + inbox[0, part].astype(f32) + inbox[1, part].astype(f32)

    def sum_args(acc, rows_of, number):
        def pieces(j, part):
            return acc[rows_of, j, 128 * part : 128 * part + 128, :]

        return pieces, column_in.at[number], column_stage.at[number]

    other_value, other_key = sum_args(dv_acc, 1 - group, 0), sum_args(dk_acc, 1 - group, 1)
    own_value, own_key = sum_args(dv_acc, group, 2), sum_args(dk_acc, group, 3)

    def mirrored_rows(name, number, args):
        for part in (0, 1):
            mirror_stage[number, 128 * part : 128 * part + 128] = column_sum(name, part, *args[:2]).astype(bf16)
        start((name, "mirror back"), mirror_stage.at[number], mirror_in.at[number], mirror)

    def own_rows(name, args, out):
        for part in (0, 1):
            out[group, 128 * part : 128 * part + 128] = column_sum(name, part, *args[:2])

    def send_dq(way, hops, part):
        number = 0 if way == "up" else 1
        device, sign = (up, 1) if way == "up" else (down, -1)
        value = dq_acc[turned(z, sign * hops, 8), halves[part]]
        if not (hops == 4 or (hops == 3 and part != number)):
            arrived(("dq", way, hops + 1, part))
            value += dq_in[number, hops, part].astype(f32)
        dq_stage[number, hops - 1, part] = value.astype(bf16)
        start(
            ("dq", way, hops, part),
            dq_stage.at[number, hops - 1, part],
            dq_in.at[number, hops - 1, part],
            device,
        )

    tile(1 - group, 7 - z, True)
    pass_query(3, 0)
    tiles(1 - group, 8 - z)
    first_columns("other value", *other_value)
    first_columns("other key", *other_key)
    tile(group, z, True)
    last_columns("other value", *other_value)
    last_columns("other key", *other_key)
    tiles(group, z + 1)
    first_columns("own value", *own_value)
    mirrored_rows("other value", 0, other_value)
    send_dq("up", 4, 0)
    send_dq("down", 4, 1)
    send_dq("up", 3, 1)
    send_dq("down", 3, 0)
    last_columns("own value", *own_value)
    first_columns("own key", *own_key)
    mirrored_rows("other key", 1, other_key)
    own_rows("own value", own_value, dv_out)
    value_narrow[group] = dv_out[group].astype(bf16)
    send_dq("up", 3, 0)
    send_dq("down", 3, 1)
    last_columns("own key", *own_key)
    arrived(("other value", "mirror back"))
    value_narrow[1 - group] = mirror_in[0]
    dv_out[1 - group] = mirror_in[0].astype(f32)

    weight_args = (lambda j, part: weight_part[j, 4 * part : 4 * part + 4]), weight_in, weight_stage
    narrow = value_narrow[...].reshape(512, 128)
    for block in range(8):
        part = lax.dot_general(latent_all[block].reshape(512, 256), narrow, cols_by_cols, preferred_element_type=f32)
        weight_part[:, block] = part.reshape(4, 64, 128)
        if block == 3:
            send_column("weight", "right", 2, 0, *weight_args)
            send_column("weight", "left", 1, 0, *weight_args)
    send_column("weight", "left", 2, 1, *weight_args)
    send_column("weight", "right", 1, 1, *weight_args)
    send_dq("up", 2, 1)
    send_dq("down", 2, 0)
    own_rows("own key", own_key, dk_out)
    send_dq("up", 2, 0)
    send_dq("down", 2, 1)
    last_columns("weight", *weight_args)
    send_dq("up", 1, 1)
    send_dq("down", 1, 0)
    for part in (0, 1):
        weight_mine[4 * part : 4 * part + 4] = column_sum("weight", part, *weight_args[:2]).astype(bf16)
    for hops in range(1, 8):
        start(("weight", hops), weight_mine.at[turned(z, hops, 8)], weight_last.at[hops - 1], others[hops - 1])
    send_dq("up", 1, 0)
    send_dq("down", 1, 1)
    arrived(("other key", "mirror back"))
    dk_out[1 - group] = mirror_in[1].astype(f32)
    for part in (0, 1):
        arrived(("dq", "up", 1, part))
        arrived(("dq", "down", 1, part))
        dq_out[halves[part]] = (
            dq_acc[z, halves[part]] + dq_in[0, 0, part].astype(f32) + dq_in[1, 0, part].astype(f32)
        )
    total = weight_mine[z].astype(f32)
    for hops in range(1, 8):
        arrived(("weight", hops))
        total += weight_last[hops - 1].astype(f32)
    weight_out[...] = total
    sender.finish()


def finish_kernel(dq_ref, dk_ref, dv_ref, weight_ref, dq_out, dk_out, dv_out, weight_out):
    dq_out[...] = 0.125 * dq_ref[...]
    dk_out[...] = 0.125 * dk_ref[...]
    dv_out[...] = dv_ref[...]
    weight_out[...] = weight_ref[...]


def per_device(queries, key_vectors, latents, w_value, log_sums, out_pair, cotangent, lambdas, out_gain):
    anywhere, vmem = pl.BlockSpec(memory_space=pl.ANY), pl.BlockSpec(memory_space=pltpu.VMEM)
    scratch = (
        ((8, 512, 256), bf16),
        ((8, 8, 512), f32),
        ((8, 2, 256, 256), bf16),
        ((2, 4, 256, 128), bf16),
        ((2, 4, 256, 128), bf16),
        ((256, 128), bf16),
        ((8, 256, 128), bf16),
        ((2, 512), f32),
        ((512, 256), bf16),
        ((512, 128), bf16),
        ((1, 128), f32),
        ((256, 128), bf16),
        ((8, 512, 128), f32),
        ((2, 4, 256, 128), f32),
        ((2, 4, 256, 128), f32),
        ((2, 4, 2, 256, 128), bf16),
        ((2, 4, 2, 256, 128), bf16),
        ((4, 2, 3, 128, 128), bf16),
        ((4, 2, 3, 128, 128), bf16),
        ((2, 256, 128), bf16),
        ((2, 256, 128), bf16),
        ((2, 256, 128), bf16),
        ((4, 8, 64, 128), f32),
        ((2, 3, 4, 64, 128), bf16),
        ((2, 3, 4, 64, 128), bf16),
        ((8, 64, 128), bf16),
        ((7, 64, 128), bf16),
    )
    sums = pl.pallas_call(
        whole_kernel,
        out_shape=(
            jax.ShapeDtypeStruct((512, 128), f32),
            jax.ShapeDtypeStruct((2, 256, 128), f32),
            jax.ShapeDtypeStruct((2, 256, 128), f32),
            jax.ShapeDtypeStruct((64, 128), f32),
        ),
        in_specs=[anywhere] * 8 + [pl.BlockSpec(memory_space=pltpu.SMEM)],
        out_specs=[vmem] * 4,
        scratch_shapes=[pltpu.VMEM(*entry) for entry in scratch]
        + [
            pltpu.SemaphoreType.DMA((9,)),
            pltpu.SemaphoreType.DMA((116,)),
            pltpu.SemaphoreType.DMA((116,)),
        ],
        compiler_params=pltpu.CompilerParams(
            collective_id=0, has_side_effects=True, vmem_limit_bytes=60 * 1024 * 1024
        ),
        name="whole",
    )(
        queries,
        key_vectors.reshape(2, 256, 128),
        latents.reshape(2, 256, 256),
        w_value.reshape(8, 256, 128),
        log_sums.T,
        out_pair,
        cotangent,
        out_gain.reshape(1, 128),
        lambdas,
    )
    query_grad, key_grad, value_grad, weight_grad = pl.pallas_call(
        finish_kernel,
        out_shape=tuple(jax.ShapeDtypeStruct(part.shape, f32) for part in sums),
        in_specs=[vmem] * 4,
        out_specs=[vmem] * 4,
        compiler_params=pltpu.CompilerParams(vmem_limit_bytes=8 * 1024 * 1024),
        name="finish",
    )(*sums)
    return query_grad, key_grad.reshape(512, 128), value_grad.reshape(512, 128), weight_grad


def solution(mesh):
    grid = Mesh(mesh.devices.reshape(8, 4, 4, 2), ("z", "x", "y", "core"))
    sp, tp = ("z", "x"), ("y", "core")
    return jax.shard_map(
        per_device,
        mesh=grid,
        in_specs=(
            P(sp, tp),
            P(sp, tp),
            P(sp, tp),
            P(None, tp),
            P(sp, tp),
            P(sp, tp),
            P(sp, tp),
            P(tp),
            P(),
        ),
        out_specs=(P(sp, tp), P(sp, tp), P(sp, tp), P(sp, tp)),
        check_vma=False,
    )
```

```python
import functools
import math

import jax
import jax.numpy as jnp
from jax import lax
from jax.experimental import pallas as pl
from jax.experimental.pallas import tpu as pltpu
from jax.sharding import Mesh, PartitionSpec as P

norm_floor = 0.25
log2_e = math.log2(math.e)
f32 = jnp.float32
bf16 = jnp.bfloat16
rows_by_rows = (((1,), (1,)), ((), ()))
rows_by_cols = (((1,), (0,)), ((), ()))
cols_by_cols = (((0,), (0,)), ((), ()))
mesh_ids = pl.DeviceIdType.MESH
tok_len = 256


class Sender:
    def __init__(self, send_sems, recv_sems):
        self.send_sems, self.recv_sems = send_sems, recv_sems
        self.copies = {}

    def plan(self, name, source, target, device):
        place = len(self.copies)
        self.copies[name] = pltpu.make_async_remote_copy(
            src_ref=source,
            dst_ref=target,
            send_sem=self.send_sems.at[place],
            recv_sem=self.recv_sems.at[place],
            device_id=device,
            device_id_type=mesh_ids,
        )

    def start(self, name):
        self.copies[name].start()

    def arrived(self, name):
        self.copies[name].wait_recv()

    def finish(self):
        for copy in self.copies.values():
            copy.wait_send()


def greet(devices):
    barrier = pltpu.get_barrier_semaphore()
    for device in devices:
        pl.semaphore_signal(barrier, inc=1, device_id=device, device_id_type=mesh_ids)
    pl.semaphore_wait(barrier, len(devices))


def turned(index, step, size):
    return lax.rem(index + (step + size), size)


def whole_kernel(
    query_hbm, key_hbm, latent_hbm, weight_hbm, log_hbm, pair_hbm, cotangent_hbm, gain_hbm, lam_ref,
    dq_out, dk_out, dv_out, weight_out,
    query_all, grad_all, row_all, latent_all, key_all, value_all,
    maps, key_given, weight_ref, log_ref, pair_ref, cotangent_ref, gain_ref, value_own,
    dq_acc, dk_acc, dv_acc, dq_in, dq_stage, column_in, column_stage,
    mirror_stage, mirror_in, value_narrow,
    weight_part, weight_stage, weight_in, weight_mine, weight_last,
    local_sems, send_sems, recv_sems,
):
    z, x, y, core = (lax.axis_index(name) for name in ("z", "x", "y", "core"))
    group = jnp.where(z < 4, 0, 1)
    half = group
    own_slot = y * 2 + core

    loads = {}
    for place, (name, source, target) in enumerate(
        (
            ("latent", latent_hbm, latent_all.at[own_slot]),
            ("key", key_hbm.at[half], key_all.at[group, x]),
            ("given", key_hbm.at[1 - half], key_given),
            ("pair", pair_hbm, pair_ref),
            ("cotangent", cotangent_hbm, cotangent_ref),
            ("gain", gain_hbm, gain_ref),
            ("log", log_hbm, log_ref),
            ("query", query_hbm, query_all.at[z]),
            ("weight", weight_hbm, weight_ref),
        )
    ):
        loads[name] = pltpu.make_async_copy(source, target, local_sems.at[place])
        loads[name].start()

    others = [{"z": turned(z, hops, 8)} for hops in range(1, 8)]
    up, down, mirror = others[0], others[6], {"z": 7 - z}
    right, left = {"x": turned(x, 1, 4)}, {"x": turned(x, -1, 4)}
    ahead, behind = {"y": turned(y, 1, 4)}, {"y": turned(y, -1, 4)}
    partner = {"core": 1 - core}
    greet(others + [right, left, ahead, behind, partner])
    sender = Sender(send_sems, recv_sems)
    plan, start, arrived = sender.plan, sender.start, sender.arrived
    halves = (pl.ds(0, 256), pl.ds(256, 256))

    def latent_slot(step, toks, part=None):
        slot = latent_all.at[turned(y, step, 4) * 2 + core, toks]
        return slot if part is None else slot.at[:, pl.ds(128 * part, 128)]

    sides = {"ahead": (ahead, -1, 0), "behind": (behind, 1, 1)}
    for name, toks in (("given", 1 - half), ("own", half)):
        for way, (device, step, far) in sides.items():
            for part in (0, 1):
                plan((name, way, part), latent_slot(0, toks, part), latent_slot(0, toks, part), device)
            plan((name, way, "far"), latent_slot(step, toks, far), latent_slot(step, toks, far), device)
        for step in (0, -1, 1, 2):
            plan(("pair", name, step), latent_slot(step, toks), latent_slot(step, toks), partner)
    for way, device, sign in (("up", up, -1), ("down", down, 1)):
        for hops in range(4):
            index = turned(z, sign * hops, 8)
            for part in (0, 1):
                if hops < 3 or (way == "up") == (part == 0):
                    slot = (query_all, grad_all)[part].at[index]
                    plan((way, hops, part), slot, slot, device)
            if hops < 3 or way == "up":
                plan((way, hops, "rows"), row_all.at[index], row_all.at[index], device)
    for name, given, target in (("key", key_given, key_all), ("value", value_own, value_all)):
        own, other = target.at[group, x], target.at[1 - group, x]
        plan((name, "mirror"), given, own, mirror)
        for way, device, step in (("right", right, -1), ("left", left, 1)):
            plan((name, "own", way), own, own, device)
            plan((name, "other", way), other, other, device)
        own, other = target.at[group, turned(x, -1, 4)], target.at[1 - group, turned(x, 1, 4)]
        plan((name, "own", "far"), own, own, right)
        plan((name, "other", "far"), other, other, left)
    for name, inbox, stages in (
        ("other value", column_in.at[0], column_stage.at[0]),
        ("own value", column_in.at[1], column_stage.at[1]),
        ("other key", column_in.at[2], column_stage.at[2]),
        ("own key", column_in.at[3], column_stage.at[3]),
        ("weight", weight_in, weight_stage),
    ):
        for number, (way, device) in enumerate((("right", right), ("left", left))):
            plan((name, way, 2, number), stages.at[number, 0], inbox.at[number, 2], device)
            plan((name, way, 1, 1 - number), stages.at[number, 1], inbox.at[number, 1 - number], device)
            plan((name, way, 1, number), stages.at[number, 2], inbox.at[number, number], device)
    for number in (0, 1):
        plan(("mirror back", number), mirror_stage.at[number], mirror_in.at[number], mirror)
    for number, (way, device) in enumerate((("up", up), ("down", down))):
        for hops in (4, 3, 2, 1):
            for part in (0, 1):
                if hops < 4 or part == number:
                    place = number, hops - 1, part
                    plan(("dq", way, hops, part), dq_stage.at[place], dq_in.at[place], device)
    for hops in range(1, 8):
        plan(("weight", hops), weight_mine.at[turned(z, hops, 8)], weight_last.at[hops - 1], others[hops - 1])

    def open_latents(name):
        for part in (0, 1):
            start((name, "ahead", part))
            start((name, "behind", 1 - part))
        start(("pair", name, 0))

    def latents_far(name):
        for way, (_, _, far) in sides.items():
            arrived((name, way, far))
            start((name, way, "far"))

    def latents_near(name):
        for way, (_, step, far) in sides.items():
            arrived((name, way, 1 - far))
            start(("pair", name, step))

    def latents_last(name):
        arrived((name, "ahead", "far"))
        arrived((name, "behind", "far"))
        start(("pair", name, 2))

    def values_of(name, toks):
        for step in (0, -1, 1, 2):
            arrived(("pair", name, step))
        total = jnp.zeros((256, 128), f32)
        for slot in range(8):
            total += jnp.dot(latent_all[slot, toks], weight_ref[slot], preferred_element_type=f32)
        return total.astype(bf16)

    def send_query(hops, part):
        for way in ("up", "down"):
            if (way, hops, part) in sender.copies:
                start((way, hops, part))
            if part == 1 and (way, hops, "rows") in sender.copies:
                start((way, hops, "rows"))

    def pass_query(hops, part):
        for way in ("up", "down"):
            if (way, hops, part) in sender.copies:
                arrived((way, hops, part))
                if (way, hops + 1, part) in sender.copies:
                    start((way, hops + 1, part))
            if part == 1 and (way, hops, "rows") in sender.copies:
                arrived((way, hops, "rows"))
                if (way, hops + 1, "rows") in sender.copies:
                    start((way, hops + 1, "rows"))

    def share_own(name):
        start((name, "own", "right"))
        start((name, "own", "left"))

    def share_mirrored(name):
        arrived((name, "mirror"))
        start((name, "other", "left"))
        start((name, "other", "right"))

    def share_far(name):
        arrived((name, "own", "right"))
        start((name, "own", "far"))
        arrived((name, "other", "left"))
        start((name, "other", "far"))

    def close_share(name):
        for which, way in (("own", "left"), ("other", "right"), ("own", "far"), ("other", "far")):
            arrived((name, which, way))

    loads["latent"].wait()
    open_latents("given")
    loads["key"].wait()
    loads["given"].wait()
    start(("key", "mirror"))
    share_own("key")
    loads["query"].wait()
    send_query(0, 0)

    for name in ("pair", "cotangent", "gain", "log"):
        loads[name].wait()
    lam = lam_ref[0]
    first_out, second_out = pair_ref[:, 0:128].astype(f32), pair_ref[:, 128:256].astype(f32)
    merged = first_out - lam * second_out
    inv_norm = lax.rsqrt(jnp.mean(merged * merged, axis=-1, keepdims=True) + norm_floor)
    scaled = cotangent_ref[...].astype(f32) * gain_ref[...]
    inner_dot = jnp.mean(scaled * merged, axis=-1, keepdims=True)
    out_grad = (inv_norm * scaled - merged * (inv_norm * inv_norm * inv_norm) * inner_dot).astype(bf16)
    grad_all[z] = out_grad
    wide = out_grad.astype(f32)
    first_term = jnp.sum(wide * first_out, axis=-1, keepdims=True)
    second_term = jnp.sum(wide * second_out, axis=-1, keepdims=True)
    lane = lax.broadcasted_iota(jnp.int32, (1, 128), 1)
    terms = jnp.where(lane == 0, first_term, second_term).T
    log_lam = jnp.log(jnp.full((1, 512), lam, f32)) * log2_e
    row_all[z, 2:4, :] = terms[0:2]
    row_all[z, 0:1, :] = log_ref[0:1, :] * log2_e
    row_all[z, 1:2, :] = log_ref[1:2, :] * log2_e - log_lam
    send_query(0, 1)

    dq_acc[...] = jnp.zeros_like(dq_acc)
    dk_acc[...] = jnp.zeros_like(dk_acc)
    dv_acc[...] = jnp.zeros_like(dv_acc)

    latents_far("given")
    open_latents("own")
    share_mirrored("key")
    latents_near("given")
    latents_last("given")
    loads["weight"].wait()
    pass_query(0, 0)
    value_own[...] = values_of("given", 1 - half)
    start(("value", "mirror"))
    share_far("key")
    latents_far("own")
    pass_query(0, 1)
    latents_near("own")
    close_share("key")

    first_lanes = lane < 64

    def split(value):
        zero = jnp.zeros_like(value)
        return jnp.where(first_lanes, value, zero), jnp.where(first_lanes, zero, value)

    def block_at(count):
        hops = (count + 1) // 2
        return turned(z, jnp.where(count % 2 == 1, -hops, hops), 8)

    def both_groups(block, work):
        def one(number, carry):
            own = number == 1
            part = jnp.where(own, group, 1 - group)
            row = jnp.where(own, z, 7 - z)
            slot = jnp.where(own, block + 1, block - 7 + z)
            pl.when(block >= row)(lambda: work(part, row, slot))
            return carry

        lax.fori_loop(0, 2, one, 0)

    def maps_tile(part, block, slot, masked):
        key_0, key_1 = split(key_all[part].reshape(1024, 128))
        for tok in range(0, 512, tok_len):
            toks = slice(tok, tok + tok_len)
            query, grad = query_all[block, toks], grad_all[block, toks]
            score_0 = lax.dot_general(key_0, query, rows_by_rows, preferred_element_type=f32)
            score_1 = lax.dot_general(key_1, query, rows_by_rows, preferred_element_type=f32)
            map_0 = jnp.exp2(score_0 * (log2_e / 8) - row_all[block, 0:1, toks])
            map_1 = jnp.exp2(score_1 * (log2_e / 8) - row_all[block, 1:2, toks])
            if masked:
                row = lax.broadcasted_iota(jnp.int32, (1024, 1), 0)
                key_pos = (row // 256 - x) * 512 + half * 256 + row % 256
                tok_pos = lax.broadcasted_iota(jnp.int32, (1, tok_len), 1) + tok
                visible = key_pos <= tok_pos
                map_0 = jnp.where(visible, map_0, 0.0)
                map_1 = jnp.where(visible, map_1, 0.0)
            maps[slot, 0, :, toks] = map_0.astype(bf16)
            maps[slot, 1, :, toks] = map_1.astype(bf16)
            mixed = (map_0 - map_1).astype(bf16)
            dv = lax.dot_general(mixed, grad, rows_by_cols, preferred_element_type=f32)
            dv_acc[part] += dv.reshape(4, 256, 128)

    def grads_tile(part, block, slot):
        key_0, key_1 = split(key_all[part].reshape(1024, 128))
        value = value_all[part].reshape(1024, 128)
        for tok in range(0, 512, tok_len):
            toks = slice(tok, tok + tok_len)
            query_0, query_1 = split(query_all[block, toks])
            dot = lax.dot_general(value, grad_all[block, toks], rows_by_rows, preferred_element_type=f32)
            map_0, map_1 = maps[slot, 0, :, toks].astype(f32), maps[slot, 1, :, toks].astype(f32)
            grad_0 = (map_0 * (dot - row_all[block, 2:3, toks])).astype(bf16)
            grad_1 = (map_1 * (row_all[block, 3:4, toks] - dot)).astype(bf16)
            dk = lax.dot_general(
                grad_0, query_0, rows_by_cols, preferred_element_type=f32
            ) + lax.dot_general(grad_1, query_1, rows_by_cols, preferred_element_type=f32)
            dk_acc[part] += dk.reshape(4, 256, 128)
            dq = lax.dot_general(
                key_0, grad_0, cols_by_cols, preferred_element_type=f32
            ) + lax.dot_general(key_1, grad_1, cols_by_cols, preferred_element_type=f32)
            dq_acc[block, toks, :] += dq.T

    def send_column(name, way, hops, part, pieces, inbox, stages):
        number, sign = (0, 1) if way == "right" else (1, -1)
        value = pieces(turned(x, sign * hops, 4), part)
        place = 0 if hops == 2 else 1
        if hops == 1 and part == number:
            arrived((name, way, 2, part))
            value += inbox[number, 2].astype(f32)
            place = 2
        stages[number, place] = value.astype(bf16)
        start((name, way, hops, part))

    def first_columns(name, *args):
        send_column(name, "right", 2, 0, *args)
        send_column(name, "left", 2, 1, *args)
        send_column(name, "right", 1, 1, *args)
        send_column(name, "left", 1, 0, *args)

    def last_columns(name, *args):
        send_column(name, "right", 1, 0, *args)
        send_column(name, "left", 1, 1, *args)

    def column_sum(name, part, pieces, inbox):
        arrived((name, "right", 1, part))
        arrived((name, "left", 1, part))
        return pieces(x, part) + inbox[0, part].astype(f32) + inbox[1, part].astype(f32)

    def sum_args(acc, rows_of, number):
        def pieces(j, part):
            return acc[rows_of, j, 128 * part : 128 * part + 128, :]

        return pieces, column_in.at[number], column_stage.at[number]

    other_value, own_value = sum_args(dv_acc, 1 - group, 0), sum_args(dv_acc, group, 1)
    other_key, own_key = sum_args(dk_acc, 1 - group, 2), sum_args(dk_acc, group, 3)
    weight_args = (lambda j, part: weight_part[j, 4 * part : 4 * part + 4]), weight_in, weight_stage

    def mirrored_rows(name, number, args):
        for part in (0, 1):
            mirror_stage[number, 128 * part : 128 * part + 128] = column_sum(name, part, *args[:2]).astype(bf16)
        start(("mirror back", number))

    def own_rows(name, args, out):
        for part in (0, 1):
            out[group, 128 * part : 128 * part + 128] = column_sum(name, part, *args[:2])

    def send_dq(way, hops):
        number, sign = (0, 1) if way == "up" else (1, -1)
        for part in (number, 1 - number):
            if hops == 4 and part != number:
                continue
            value = dq_acc[turned(z, sign * hops, 8), halves[part]]
            if hops < 3 or (hops == 3 and part == number):
                arrived(("dq", way, hops + 1, part))
                value += dq_in[number, hops, part].astype(f32)
            dq_stage[number, hops - 1, part] = value.astype(bf16)
            start(("dq", way, hops, part))

    def maps_step(count, carry):
        @pl.when(count == 1)
        def _():
            latents_last("own")
            value_all[group, x] = values_of("own", half)
            share_own("value")

        @pl.when(count == 2)
        def _():
            pass_query(1, 0)
            share_mirrored("value")

        @pl.when(count == 3)
        def _():
            pass_query(1, 1)
            share_far("value")

        pl.when(count == 4)(lambda: pass_query(2, 0))
        pl.when(count == 5)(lambda: pass_query(2, 1))

        @pl.when(count == 7)
        def _():
            pass_query(3, 0)
            pass_query(3, 1)

        block = block_at(count)

        def work(part, row, slot):
            pl.when(block == row)(lambda: maps_tile(part, block, slot, True))
            pl.when(block != row)(lambda: maps_tile(part, block, slot, False))

        both_groups(block, work)
        return carry

    lax.fori_loop(0, 8, maps_step, 0)
    first_columns("other value", *other_value)
    first_columns("own value", *own_value)
    close_share("value")

    def values_summed():
        mirrored_rows("other value", 0, other_value)
        own_rows("own value", own_value, dv_out)
        value_narrow[group] = dv_out[group].astype(bf16)

    def weights_made():
        arrived(("mirror back", 0))
        value_narrow[1 - group] = mirror_in[0]
        dv_out[1 - group] = mirror_in[0].astype(f32)
        narrow = value_narrow[...].reshape(512, 128)
        for block in range(8):
            part = lax.dot_general(
                latent_all[block].reshape(512, 256), narrow, cols_by_cols, preferred_element_type=f32
            )
            weight_part[:, block] = part.reshape(4, 64, 128)
            if block == 3:
                send_column("weight", "right", 2, 0, *weight_args)
                send_column("weight", "left", 1, 0, *weight_args)
        send_column("weight", "left", 2, 1, *weight_args)
        send_column("weight", "right", 1, 1, *weight_args)

    def weights_summed():
        for part in (0, 1):
            weight_mine[4 * part : 4 * part + 4] = column_sum("weight", part, *weight_args[:2]).astype(bf16)
        for hops in (4, 3, 5, 2, 6, 1, 7):
            start(("weight", hops))

    def grads_step(count, carry):
        block = block_at(7 - count)
        both_groups(block, lambda part, row, slot: grads_tile(part, block, slot))

        @pl.when(count == 0)
        def _():
            last_columns("other value", *other_value)
            last_columns("own value", *own_value)
            send_dq("up", 4)
            send_dq("down", 4)

        @pl.when(count == 1)
        def _():
            send_dq("up", 3)

        @pl.when(count == 2)
        def _():
            values_summed()
            send_dq("down", 3)

        pl.when(count == 3)(lambda: send_dq("up", 2))

        @pl.when(count == 4)
        def _():
            weights_made()
            send_dq("down", 2)

        pl.when(count == 5)(lambda: send_dq("up", 1))

        @pl.when(count == 6)
        def _():
            last_columns("weight", *weight_args)
            send_dq("down", 1)

        return carry

    lax.fori_loop(0, 8, grads_step, 0)
    first_columns("other key", *other_key)
    first_columns("own key", *own_key)
    weights_summed()
    last_columns("other key", *other_key)
    last_columns("own key", *own_key)
    for part in (0, 1):
        arrived(("dq", "up", 1, part))
        arrived(("dq", "down", 1, part))
        dq_out[halves[part]] = (
            dq_acc[z, halves[part]] + dq_in[0, 0, part].astype(f32) + dq_in[1, 0, part].astype(f32)
        )
    mirrored_rows("other key", 1, other_key)
    own_rows("own key", own_key, dk_out)
    total = weight_mine[z].astype(f32)
    for hops in range(1, 8):
        arrived(("weight", hops))
        total += weight_last[hops - 1].astype(f32)
    weight_out[...] = total
    arrived(("mirror back", 1))
    dk_out[1 - group] = mirror_in[1].astype(f32)
    sender.finish()


def finish_kernel(*refs):
    sums, outs, held, load_sems, store_sems = refs[:4], refs[4:8], refs[8:12], refs[12], refs[13]
    loads = [pltpu.make_async_copy(sums[i], held[i], load_sems.at[i]) for i in range(4)]
    stores = [pltpu.make_async_copy(held[i], outs[i], store_sems.at[i]) for i in range(4)]
    for load in loads:
        load.start()
    for i in (3, 2):
        loads[i].wait()
        stores[i].start()
    for i in (0, 1):
        loads[i].wait()
        held[i][...] = 0.125 * held[i][...]
        stores[i].start()
    for store in stores:
        store.wait()


def per_device(queries, key_vectors, latents, w_value, log_sums, out_pair, cotangent, lambdas, out_gain):
    anywhere, vmem = pl.BlockSpec(memory_space=pl.ANY), pl.BlockSpec(memory_space=pltpu.VMEM)
    scratch = (
        ((8, 512, 128), bf16),
        ((8, 512, 128), bf16),
        ((8, 4, 512), f32),
        ((8, 2, 256, 256), bf16),
        ((2, 4, 256, 128), bf16),
        ((2, 4, 256, 128), bf16),
        ((9, 2, 1024, 512), bf16),
        ((256, 128), bf16),
        ((8, 256, 128), bf16),
        ((2, 512), f32),
        ((512, 256), bf16),
        ((512, 128), bf16),
        ((1, 128), f32),
        ((256, 128), bf16),
        ((8, 512, 128), f32),
        ((2, 4, 256, 128), f32),
        ((2, 4, 256, 128), f32),
        ((2, 4, 2, 256, 128), bf16),
        ((2, 4, 2, 256, 128), bf16),
        ((4, 2, 3, 128, 128), bf16),
        ((4, 2, 3, 128, 128), bf16),
        ((2, 256, 128), bf16),
        ((2, 256, 128), bf16),
        ((2, 256, 128), bf16),
        ((4, 8, 64, 128), f32),
        ((2, 3, 4, 64, 128), bf16),
        ((2, 3, 4, 64, 128), bf16),
        ((8, 64, 128), bf16),
        ((7, 64, 128), bf16),
    )
    sums = pl.pallas_call(
        whole_kernel,
        out_shape=(
            jax.ShapeDtypeStruct((512, 128), f32),
            jax.ShapeDtypeStruct((2, 256, 128), f32),
            jax.ShapeDtypeStruct((2, 256, 128), f32),
            jax.ShapeDtypeStruct((64, 128), f32),
        ),
        in_specs=[anywhere] * 8 + [pl.BlockSpec(memory_space=pltpu.SMEM)],
        out_specs=[vmem] * 4,
        scratch_shapes=[pltpu.VMEM(*entry) for entry in scratch]
        + [
            pltpu.SemaphoreType.DMA((9,)),
            pltpu.SemaphoreType.DMA((116,)),
            pltpu.SemaphoreType.DMA((116,)),
        ],
        compiler_params=pltpu.CompilerParams(
            collective_id=0, has_side_effects=True, vmem_limit_bytes=60 * 1024 * 1024
        ),
        name="whole",
    )(
        queries,
        key_vectors.reshape(2, 256, 128),
        latents.reshape(2, 256, 256),
        w_value.reshape(8, 256, 128),
        log_sums.T,
        out_pair,
        cotangent,
        out_gain.reshape(1, 128),
        lambdas,
    )
    query_grad, key_grad, value_grad, weight_grad = pl.pallas_call(
        finish_kernel,
        out_shape=tuple(jax.ShapeDtypeStruct(part.shape, f32) for part in sums),
        in_specs=[anywhere] * 4,
        out_specs=[anywhere] * 4,
        scratch_shapes=[pltpu.VMEM(part.shape, f32) for part in sums]
        + [pltpu.SemaphoreType.DMA((4,)), pltpu.SemaphoreType.DMA((4,))],
        compiler_params=pltpu.CompilerParams(vmem_limit_bytes=60 * 1024 * 1024),
        name="finish",
    )(*sums)
    return query_grad, key_grad.reshape(512, 128), value_grad.reshape(512, 128), weight_grad


def solution(mesh):
    grid = Mesh(mesh.devices.reshape(8, 4, 4, 2), ("z", "x", "y", "core"))
    sp, tp = ("z", "x"), ("y", "core")
    return jax.shard_map(
        per_device,
        mesh=grid,
        in_specs=(
            P(sp, tp),
            P(sp, tp),
            P(sp, tp),
            P(None, tp),
            P(sp, tp),
            P(sp, tp),
            P(sp, tp),
            P(tp),
            P(),
        ),
        out_specs=(P(sp, tp), P(sp, tp), P(sp, tp), P(sp, tp)),
        check_vma=False,
    )
```

```python
import functools
import math

import jax
import jax.numpy as jnp
from jax import lax
from jax.experimental import pallas as pl
from jax.experimental.pallas import tpu as pltpu
from jax.sharding import Mesh, PartitionSpec as P

norm_floor = 0.25
log2_e = math.log2(math.e)
f32 = jnp.float32
bf16 = jnp.bfloat16
rows_by_rows = (((1,), (1,)), ((), ()))
rows_by_cols = (((1,), (0,)), ((), ()))
cols_by_cols = (((0,), (0,)), ((), ()))
mesh_ids = pl.DeviceIdType.MESH
tok_len = 256


class Sender:
    def __init__(self, send_sems, recv_sems):
        self.send_sems, self.recv_sems = send_sems, recv_sems
        self.copies = {}

    def plan(self, name, source, target, device):
        place = len(self.copies)
        self.copies[name] = pltpu.make_async_remote_copy(
            src_ref=source,
            dst_ref=target,
            send_sem=self.send_sems.at[place],
            recv_sem=self.recv_sems.at[place],
            device_id=device,
            device_id_type=mesh_ids,
        )

    def start(self, name):
        self.copies[name].start()

    def arrived(self, name):
        self.copies[name].wait_recv()

    def finish(self):
        for copy in self.copies.values():
            copy.wait_send()


def greet(devices):
    barrier = pltpu.get_barrier_semaphore()
    for device in devices:
        pl.semaphore_signal(barrier, inc=1, device_id=device, device_id_type=mesh_ids)
    pl.semaphore_wait(barrier, len(devices))


def turned(index, step, size):
    return lax.rem(index + (step + size), size)


def whole_kernel(
    query_hbm, key_hbm, latent_hbm, weight_hbm, log_hbm, pair_hbm, cotangent_hbm, gain_hbm, lam_ref,
    dq_hbm, dk_hbm, dv_hbm, sum_hbm,
    query_all, grad_all, row_all, latent_all, key_all, value_all,
    dq_out, dk_out, dv_out, weight_out, maps, key_given, weight_ref, log_ref, pair_ref, cotangent_ref, gain_ref, value_own,
    dq_acc, dk_acc, dv_acc, dq_in, dq_stage, column_in, column_stage,
    mirror_stage, mirror_in, value_narrow,
    weight_part, weight_stage, weight_in, weight_mine, weight_last,
    local_sems, send_sems, recv_sems,
):
    z, x, y, core = (lax.axis_index(name) for name in ("z", "x", "y", "core"))
    group = jnp.where(z < 4, 0, 1)
    half = group
    own_slot = y * 2 + core

    loads = {}
    for place, (name, source, target) in enumerate(
        (
            ("latent", latent_hbm, latent_all.at[own_slot]),
            ("key", key_hbm.at[half], key_all.at[group, x]),
            ("given", key_hbm.at[1 - half], key_given),
            ("pair", pair_hbm, pair_ref),
            ("cotangent", cotangent_hbm, cotangent_ref),
            ("gain", gain_hbm, gain_ref),
            ("log", log_hbm, log_ref),
            ("query", query_hbm, query_all.at[z]),
            ("weight", weight_hbm, weight_ref),
        )
    ):
        loads[name] = pltpu.make_async_copy(source, target, local_sems.at[place])
        loads[name].start()

    others = [{"z": turned(z, hops, 8)} for hops in range(1, 8)]
    up, down, mirror = others[0], others[6], {"z": 7 - z}
    right, left = {"x": turned(x, 1, 4)}, {"x": turned(x, -1, 4)}
    ahead, behind = {"y": turned(y, 1, 4)}, {"y": turned(y, -1, 4)}
    partner = {"core": 1 - core}
    greet(others + [right, left, ahead, behind, partner])
    sender = Sender(send_sems, recv_sems)
    plan, start, arrived = sender.plan, sender.start, sender.arrived
    halves = (pl.ds(0, 256), pl.ds(256, 256))

    stores = {
        name: pltpu.make_async_copy(source, target, local_sems.at[9 + place])
        for place, (name, source, target) in enumerate(
            (
                ("dq0", dq_out.at[halves[0]], dq_hbm.at[halves[0]]),
                ("dq1", dq_out.at[halves[1]], dq_hbm.at[halves[1]]),
                ("dk", dk_out, dk_hbm),
                ("dv", dv_out, dv_hbm),
                ("weight", weight_out, sum_hbm),
            )
        )
    }

    def store(name):
        stores[name].start()

    def latent_slot(step, toks, part=None):
        slot = latent_all.at[turned(y, step, 4) * 2 + core, toks]
        return slot if part is None else slot.at[:, pl.ds(128 * part, 128)]

    sides = {"ahead": (ahead, -1, 0), "behind": (behind, 1, 1)}
    for name, toks in (("given", 1 - half), ("own", half)):
        for way, (device, step, far) in sides.items():
            for part in (0, 1):
                plan((name, way, part), latent_slot(0, toks, part), latent_slot(0, toks, part), device)
            plan((name, way, "far"), latent_slot(step, toks, far), latent_slot(step, toks, far), device)
        for step in (0, -1, 1, 2):
            plan(("pair", name, step), latent_slot(step, toks), latent_slot(step, toks), partner)
    for way, device, sign in (("up", up, -1), ("down", down, 1)):
        for hops in range(4):
            index = turned(z, sign * hops, 8)
            for part in (0, 1):
                if hops < 3 or (way == "up") == (part == 0):
                    slot = (query_all, grad_all)[part].at[index]
                    plan((way, hops, part), slot, slot, device)
            if hops < 3 or way == "up":
                plan((way, hops, "rows"), row_all.at[index], row_all.at[index], device)
    for name, given, target in (("key", key_given, key_all), ("value", value_own, value_all)):
        own, other = target.at[group, x], target.at[1 - group, x]
        plan((name, "mirror"), given, own, mirror)
        for way, device, step in (("right", right, -1), ("left", left, 1)):
            plan((name, "own", way), own, own, device)
            plan((name, "other", way), other, other, device)
        own, other = target.at[group, turned(x, -1, 4)], target.at[1 - group, turned(x, 1, 4)]
        plan((name, "own", "far"), own, own, right)
        plan((name, "other", "far"), other, other, left)
    for name, inbox, stages in (
        ("other value", column_in.at[0], column_stage.at[0]),
        ("own value", column_in.at[1], column_stage.at[1]),
        ("other key", column_in.at[2], column_stage.at[2]),
        ("own key", column_in.at[3], column_stage.at[3]),
        ("weight", weight_in, weight_stage),
    ):
        for number, (way, device) in enumerate((("right", right), ("left", left))):
            plan((name, way, 2, number), stages.at[number, 0], inbox.at[number, 2], device)
            plan((name, way, 1, 1 - number), stages.at[number, 1], inbox.at[number, 1 - number], device)
            plan((name, way, 1, number), stages.at[number, 2], inbox.at[number, number], device)
    for number in (0, 1):
        plan(("mirror back", number), mirror_stage.at[number], mirror_in.at[number], mirror)
    for number, (way, device) in enumerate((("up", up), ("down", down))):
        for hops in (4, 3, 2, 1):
            for part in (0, 1):
                if hops < 4 or part == number:
                    place = number, hops - 1, part
                    plan(("dq", way, hops, part), dq_stage.at[place], dq_in.at[place], device)
    for hops in range(1, 8):
        plan(("weight", hops), weight_mine.at[turned(z, hops, 8)], weight_last.at[hops - 1], others[hops - 1])

    def open_latents(name):
        for part in (0, 1):
            start((name, "ahead", part))
            start((name, "behind", 1 - part))
        start(("pair", name, 0))

    def latents_far(name):
        for way, (_, _, far) in sides.items():
            arrived((name, way, far))
            start((name, way, "far"))

    def latents_near(name):
        for way, (_, step, far) in sides.items():
            arrived((name, way, 1 - far))
            start(("pair", name, step))

    def latents_last(name):
        arrived((name, "ahead", "far"))
        arrived((name, "behind", "far"))
        start(("pair", name, 2))

    def values_of(name, toks):
        for step in (0, -1, 1, 2):
            arrived(("pair", name, step))
        total = jnp.zeros((256, 128), f32)
        for slot in range(8):
            total += jnp.dot(latent_all[slot, toks], weight_ref[slot], preferred_element_type=f32)
        return total.astype(bf16)

    def send_query(hops, part):
        for way in ("up", "down"):
            if (way, hops, part) in sender.copies:
                start((way, hops, part))
            if part == 1 and (way, hops, "rows") in sender.copies:
                start((way, hops, "rows"))

    def pass_query(hops, part):
        for way in ("up", "down"):
            if (way, hops, part) in sender.copies:
                arrived((way, hops, part))
                if (way, hops + 1, part) in sender.copies:
                    start((way, hops + 1, part))
            if part == 1 and (way, hops, "rows") in sender.copies:
                arrived((way, hops, "rows"))
                if (way, hops + 1, "rows") in sender.copies:
                    start((way, hops + 1, "rows"))

    def share_own(name):
        start((name, "own", "right"))
        start((name, "own", "left"))

    def share_mirrored(name):
        arrived((name, "mirror"))
        start((name, "other", "left"))
        start((name, "other", "right"))

    def share_far(name):
        arrived((name, "own", "right"))
        start((name, "own", "far"))
        arrived((name, "other", "left"))
        start((name, "other", "far"))

    def close_share(name):
        for which, way in (("own", "left"), ("other", "right"), ("own", "far"), ("other", "far")):
            arrived((name, which, way))

    loads["latent"].wait()
    open_latents("given")
    loads["key"].wait()
    loads["given"].wait()
    start(("key", "mirror"))
    share_own("key")
    loads["query"].wait()
    send_query(0, 0)

    for name in ("pair", "cotangent", "gain", "log"):
        loads[name].wait()
    lam = lam_ref[0]
    first_out, second_out = pair_ref[:, 0:128].astype(f32), pair_ref[:, 128:256].astype(f32)
    merged = first_out - lam * second_out
    inv_norm = lax.rsqrt(jnp.mean(merged * merged, axis=-1, keepdims=True) + norm_floor)
    scaled = cotangent_ref[...].astype(f32) * gain_ref[...]
    inner_dot = jnp.mean(scaled * merged, axis=-1, keepdims=True)
    out_grad = (inv_norm * scaled - merged * (inv_norm * inv_norm * inv_norm) * inner_dot).astype(bf16)
    grad_all[z] = out_grad
    wide = out_grad.astype(f32)
    first_term = jnp.sum(wide * first_out, axis=-1, keepdims=True)
    second_term = jnp.sum(wide * second_out, axis=-1, keepdims=True)
    lane = lax.broadcasted_iota(jnp.int32, (1, 128), 1)
    terms = jnp.where(lane == 0, first_term, second_term).T
    log_lam = jnp.log(jnp.full((1, 512), lam, f32)) * log2_e
    row_all[z, 2:4, :] = terms[0:2]
    row_all[z, 0:1, :] = log_ref[0:1, :] * log2_e
    row_all[z, 1:2, :] = log_ref[1:2, :] * log2_e - log_lam
    send_query(0, 1)

    dq_acc[...] = jnp.zeros_like(dq_acc)
    dk_acc[...] = jnp.zeros_like(dk_acc)
    dv_acc[...] = jnp.zeros_like(dv_acc)

    latents_far("given")
    open_latents("own")
    share_mirrored("key")
    pass_query(0, 0)
    latents_near("given")
    share_far("key")
    latents_last("given")
    loads["weight"].wait()
    latents_far("own")
    value_own[...] = values_of("given", 1 - half)
    start(("value", "mirror"))
    pass_query(0, 1)
    latents_near("own")
    close_share("key")

    first_lanes = lane < 64

    def split(value):
        zero = jnp.zeros_like(value)
        return jnp.where(first_lanes, value, zero), jnp.where(first_lanes, zero, value)

    def block_at(count):
        hops = (count + 1) // 2
        return turned(z, jnp.where(count % 2 == 1, -hops, hops), 8)

    def both_groups(block, work):
        def one(number, carry):
            own = number == 1
            part = jnp.where(own, group, 1 - group)
            row = jnp.where(own, z, 7 - z)
            slot = jnp.where(own, block + 1, block - 7 + z)
            pl.when(block >= row)(lambda: work(part, row, slot))
            return carry

        lax.fori_loop(0, 2, one, 0)

    def maps_tile(part, block, slot, masked):
        key_0, key_1 = split(key_all[part].reshape(1024, 128))
        for tok in range(0, 512, tok_len):
            toks = slice(tok, tok + tok_len)
            query, grad = query_all[block, toks], grad_all[block, toks]
            score_0 = lax.dot_general(key_0, query, rows_by_rows, preferred_element_type=f32)
            score_1 = lax.dot_general(key_1, query, rows_by_rows, preferred_element_type=f32)
            map_0 = jnp.exp2(score_0 * (log2_e / 8) - row_all[block, 0:1, toks])
            map_1 = jnp.exp2(score_1 * (log2_e / 8) - row_all[block, 1:2, toks])
            if masked:
                row = lax.broadcasted_iota(jnp.int32, (1024, 1), 0)
                key_pos = (row // 256 - x) * 512 + half * 256 + row % 256
                tok_pos = lax.broadcasted_iota(jnp.int32, (1, tok_len), 1) + tok
                visible = key_pos <= tok_pos
                map_0 = jnp.where(visible, map_0, 0.0)
                map_1 = jnp.where(visible, map_1, 0.0)
            maps[slot, 0, :, toks] = map_0.astype(bf16)
            maps[slot, 1, :, toks] = map_1.astype(bf16)
            mixed = (map_0 - map_1).astype(bf16)
            dv = lax.dot_general(mixed, grad, rows_by_cols, preferred_element_type=f32)
            dv_acc[part] += dv.reshape(4, 256, 128)

    def grads_tile(part, block, slot):
        key_0, key_1 = split(key_all[part].reshape(1024, 128))
        value = value_all[part].reshape(1024, 128)
        for tok in range(0, 512, tok_len):
            toks = slice(tok, tok + tok_len)
            query_0, query_1 = split(query_all[block, toks])
            dot = lax.dot_general(value, grad_all[block, toks], rows_by_rows, preferred_element_type=f32)
            map_0, map_1 = maps[slot, 0, :, toks].astype(f32), maps[slot, 1, :, toks].astype(f32)
            grad_0 = (map_0 * (dot - row_all[block, 2:3, toks])).astype(bf16)
            grad_1 = (map_1 * (row_all[block, 3:4, toks] - dot)).astype(bf16)
            dk = lax.dot_general(
                grad_0, query_0, rows_by_cols, preferred_element_type=f32
            ) + lax.dot_general(grad_1, query_1, rows_by_cols, preferred_element_type=f32)
            dk_acc[part] += dk.reshape(4, 256, 128)
            dq = lax.dot_general(
                key_0, grad_0, cols_by_cols, preferred_element_type=f32
            ) + lax.dot_general(key_1, grad_1, cols_by_cols, preferred_element_type=f32)
            dq_acc[block, toks, :] += dq.T

    def send_column(name, way, hops, part, pieces, inbox, stages):
        number, sign = (0, 1) if way == "right" else (1, -1)
        value = pieces(turned(x, sign * hops, 4), part)
        place = 0 if hops == 2 else 1
        if hops == 1 and part == number:
            arrived((name, way, 2, part))
            value += inbox[number, 2].astype(f32)
            place = 2
        stages[number, place] = value.astype(bf16)
        start((name, way, hops, part))

    def first_columns(name, *args):
        send_column(name, "right", 2, 0, *args)
        send_column(name, "left", 2, 1, *args)
        send_column(name, "right", 1, 1, *args)
        send_column(name, "left", 1, 0, *args)

    def last_columns(name, *args):
        send_column(name, "right", 1, 0, *args)
        send_column(name, "left", 1, 1, *args)

    def column_sum(name, part, pieces, inbox):
        arrived((name, "right", 1, part))
        arrived((name, "left", 1, part))
        return pieces(x, part) + inbox[0, part].astype(f32) + inbox[1, part].astype(f32)

    def sum_args(acc, rows_of, number):
        def pieces(j, part):
            return acc[rows_of, j, 128 * part : 128 * part + 128, :]

        return pieces, column_in.at[number], column_stage.at[number]

    other_value, own_value = sum_args(dv_acc, 1 - group, 0), sum_args(dv_acc, group, 1)
    other_key, own_key = sum_args(dk_acc, 1 - group, 2), sum_args(dk_acc, group, 3)
    weight_args = (lambda j, part: weight_part[j, 4 * part : 4 * part + 4]), weight_in, weight_stage

    def mirrored_rows(name, number, args):
        for part in (0, 1):
            mirror_stage[number, 128 * part : 128 * part + 128] = column_sum(name, part, *args[:2]).astype(bf16)
        start(("mirror back", number))

    def own_rows(name, args, out):
        for part in (0, 1):
            out[group, 128 * part : 128 * part + 128] = column_sum(name, part, *args[:2])

    def send_dq(way, hops, part):
        number, sign = (0, 1) if way == "up" else (1, -1)
        value = dq_acc[turned(z, sign * hops, 8), halves[part]]
        if hops < 3 or (hops == 3 and part == number):
            arrived(("dq", way, hops + 1, part))
            value += dq_in[number, hops, part].astype(f32)
        dq_stage[number, hops - 1, part] = value.astype(bf16)
        start(("dq", way, hops, part))

    def maps_step(count, carry):
        @pl.when(count == 1)
        def _():
            latents_last("own")
            value_all[group, x] = values_of("own", half)
            share_own("value")

        @pl.when(count == 2)
        def _():
            pass_query(1, 0)
            share_mirrored("value")

        @pl.when(count == 3)
        def _():
            pass_query(1, 1)
            share_far("value")

        pl.when(count == 4)(lambda: pass_query(2, 0))
        pl.when(count == 5)(lambda: pass_query(2, 1))

        @pl.when(count == 7)
        def _():
            pass_query(3, 0)
            pass_query(3, 1)

        block = block_at(count)

        def work(part, row, slot):
            pl.when(block == row)(lambda: maps_tile(part, block, slot, True))
            pl.when(block != row)(lambda: maps_tile(part, block, slot, False))

        both_groups(block, work)
        return carry

    lax.fori_loop(0, 8, maps_step, 0)
    first_columns("other value", *other_value)
    close_share("value")

    def weights_made():
        arrived(("mirror back", 0))
        value_narrow[1 - group] = mirror_in[0]
        dv_out[1 - group] = mirror_in[0].astype(f32)
        narrow = value_narrow[...].reshape(512, 128)
        for block in range(8):
            part = lax.dot_general(
                latent_all[block].reshape(512, 256), narrow, cols_by_cols, preferred_element_type=f32
            )
            weight_part[:, block] = part.reshape(4, 64, 128)
            if block == 3:
                send_column("weight", "right", 2, 0, *weight_args)
                send_column("weight", "left", 1, 0, *weight_args)
        send_column("weight", "left", 2, 1, *weight_args)
        send_column("weight", "right", 1, 1, *weight_args)

    def weights_summed():
        for part in (0, 1):
            weight_mine[4 * part : 4 * part + 4] = column_sum("weight", part, *weight_args[:2]).astype(bf16)
        for hops in (4, 3, 5, 2, 6, 1, 7):
            start(("weight", hops))

    def tile_at(count):
        found, passed = jnp.int32(0), jnp.int32(0)
        for row in (7 - z, z):
            for hops in (4, 3, 5, 2, 6, 1, 7, 0):
                block = turned(z, hops, 8)
                counts = block >= row
                found = jnp.where(counts & (passed == count), block, found)
                passed = passed + jnp.where(counts, 1, 0)
        return found

    def grads_step(count, carry):
        other = count <= z
        block = tile_at(count)
        part = jnp.where(other, 1 - group, group)
        grads_tile(part, block, jnp.where(other, block - 7 + z, block + 1))

        @pl.when(count == 1)
        def _():
            last_columns("other value", *other_value)
            first_columns("own value", *own_value)

        @pl.when(count == 3)
        def _():
            mirrored_rows("other value", 0, other_value)
            last_columns("own value", *own_value)

        @pl.when(count == 5)
        def _():
            send_dq("up", 4, 0)
            send_dq("down", 4, 1)
            send_dq("up", 3, 1)
            send_dq("down", 3, 0)
            own_rows("own value", own_value, dv_out)
            value_narrow[group] = dv_out[group].astype(bf16)

        pl.when(count == 6)(weights_made)

        @pl.when(count == 7)
        def _():
            send_dq("up", 3, 0)
            send_dq("down", 3, 1)
            send_dq("up", 2, 1)
            send_dq("down", 2, 0)

        pl.when(count == z)(lambda: first_columns("other key", *other_key))
        pl.when((count == z + 2) & (z < 6))(lambda: last_columns("other key", *other_key))
        pl.when((count == z + 4) & (z < 4))(lambda: mirrored_rows("other key", 1, other_key))
        return carry

    lax.fori_loop(0, 9, grads_step, 0)
    first_columns("own key", *own_key)
    store("dv")
    pl.when(z >= 6)(lambda: last_columns("other key", *other_key))
    last_columns("weight", *weight_args)
    send_dq("up", 2, 0)
    send_dq("down", 2, 1)
    send_dq("up", 1, 1)
    send_dq("down", 1, 0)
    last_columns("own key", *own_key)
    pl.when(z >= 4)(lambda: mirrored_rows("other key", 1, other_key))
    weights_summed()
    send_dq("up", 1, 0)
    send_dq("down", 1, 1)
    own_rows("own key", own_key, dk_out)
    arrived(("mirror back", 1))
    dk_out[1 - group] = mirror_in[1].astype(f32)
    store("dk")
    for part in (0, 1):
        arrived(("dq", "up", 1, part))
        arrived(("dq", "down", 1, part))
        dq_out[halves[part]] = (
            dq_acc[z, halves[part]] + dq_in[0, 0, part].astype(f32) + dq_in[1, 0, part].astype(f32)
        )
        store("dq" + str(part))
    total = weight_mine[z].astype(f32)
    for hops in range(1, 8):
        arrived(("weight", hops))
        total += weight_last[hops - 1].astype(f32)
    weight_out[...] = total
    store("weight")
    for copy in stores.values():
        copy.wait()
    sender.finish()


def finish_kernel(*refs):
    sums, outs, held, load_sems, store_sems = refs[:4], refs[4:8], refs[8:12], refs[12], refs[13]
    loads = [pltpu.make_async_copy(sums[i], held[i], load_sems.at[i]) for i in range(4)]
    stores = [pltpu.make_async_copy(held[i], outs[i], store_sems.at[i]) for i in range(4)]
    for load in loads:
        load.start()
    for i in (3, 2):
        loads[i].wait()
        stores[i].start()
    for i in (0, 1):
        loads[i].wait()
        held[i][...] = 0.125 * held[i][...]
        stores[i].start()
    for store in stores:
        store.wait()


def per_device(queries, key_vectors, latents, w_value, log_sums, out_pair, cotangent, lambdas, out_gain):
    anywhere = pl.BlockSpec(memory_space=pl.ANY)
    scratch = (
        ((8, 512, 128), bf16),
        ((8, 512, 128), bf16),
        ((8, 4, 512), f32),
        ((8, 2, 256, 256), bf16),
        ((2, 4, 256, 128), bf16),
        ((2, 4, 256, 128), bf16),
        ((512, 128), f32),
        ((2, 256, 128), f32),
        ((2, 256, 128), f32),
        ((64, 128), f32),
        ((9, 2, 1024, 512), bf16),
        ((256, 128), bf16),
        ((8, 256, 128), bf16),
        ((2, 512), f32),
        ((512, 256), bf16),
        ((512, 128), bf16),
        ((1, 128), f32),
        ((256, 128), bf16),
        ((8, 512, 128), f32),
        ((2, 4, 256, 128), f32),
        ((2, 4, 256, 128), f32),
        ((2, 4, 2, 256, 128), bf16),
        ((2, 4, 2, 256, 128), bf16),
        ((4, 2, 3, 128, 128), bf16),
        ((4, 2, 3, 128, 128), bf16),
        ((2, 256, 128), bf16),
        ((2, 256, 128), bf16),
        ((2, 256, 128), bf16),
        ((4, 8, 64, 128), f32),
        ((2, 3, 4, 64, 128), bf16),
        ((2, 3, 4, 64, 128), bf16),
        ((8, 64, 128), bf16),
        ((7, 64, 128), bf16),
    )
    sums = pl.pallas_call(
        whole_kernel,
        out_shape=(
            jax.ShapeDtypeStruct((512, 128), f32),
            jax.ShapeDtypeStruct((2, 256, 128), f32),
            jax.ShapeDtypeStruct((2, 256, 128), f32),
            jax.ShapeDtypeStruct((64, 128), f32),
        ),
        in_specs=[anywhere] * 8 + [pl.BlockSpec(memory_space=pltpu.SMEM)],
        out_specs=[anywhere] * 4,
        scratch_shapes=[pltpu.VMEM(*entry) for entry in scratch]
        + [
            pltpu.SemaphoreType.DMA((14,)),
            pltpu.SemaphoreType.DMA((116,)),
            pltpu.SemaphoreType.DMA((116,)),
        ],
        compiler_params=pltpu.CompilerParams(
            collective_id=0, has_side_effects=True, vmem_limit_bytes=60 * 1024 * 1024
        ),
        name="whole",
    )(
        queries,
        key_vectors.reshape(2, 256, 128),
        latents.reshape(2, 256, 256),
        w_value.reshape(8, 256, 128),
        log_sums.T,
        out_pair,
        cotangent,
        out_gain.reshape(1, 128),
        lambdas,
    )
    query_grad, key_grad, value_grad, weight_grad = pl.pallas_call(
        finish_kernel,
        out_shape=tuple(jax.ShapeDtypeStruct(part.shape, f32) for part in sums),
        in_specs=[anywhere] * 4,
        out_specs=[anywhere] * 4,
        scratch_shapes=[pltpu.VMEM(part.shape, f32) for part in sums]
        + [pltpu.SemaphoreType.DMA((4,)), pltpu.SemaphoreType.DMA((4,))],
        compiler_params=pltpu.CompilerParams(vmem_limit_bytes=60 * 1024 * 1024),
        name="finish",
    )(*sums)
    return query_grad, key_grad.reshape(512, 128), value_grad.reshape(512, 128), weight_grad


def solution(mesh):
    grid = Mesh(mesh.devices.reshape(8, 4, 4, 2), ("z", "x", "y", "core"))
    sp, tp = ("z", "x"), ("y", "core")
    return jax.shard_map(
        per_device,
        mesh=grid,
        in_specs=(
            P(sp, tp),
            P(sp, tp),
            P(sp, tp),
            P(None, tp),
            P(sp, tp),
            P(sp, tp),
            P(sp, tp),
            P(tp),
            P(),
        ),
        out_specs=(P(sp, tp), P(sp, tp), P(sp, tp), P(sp, tp)),
        check_vma=False,
    )
```

```python
import functools
import math

import jax
import jax.numpy as jnp
from jax import lax
from jax.experimental import pallas as pl
from jax.experimental.pallas import tpu as pltpu
from jax.sharding import Mesh, PartitionSpec as P

norm_floor = 0.25
log2_e = math.log2(math.e)
f32 = jnp.float32
bf16 = jnp.bfloat16
rows_by_rows = (((1,), (1,)), ((), ()))
rows_by_cols = (((1,), (0,)), ((), ()))
cols_by_cols = (((0,), (0,)), ((), ()))
mesh_ids = pl.DeviceIdType.MESH
tok_len = 512


class Sender:
    def __init__(self, send_sems, recv_sems):
        self.send_sems, self.recv_sems = send_sems, recv_sems
        self.copies = {}

    def plan(self, name, source, target, device):
        place = len(self.copies)
        self.copies[name] = pltpu.make_async_remote_copy(
            src_ref=source,
            dst_ref=target,
            send_sem=self.send_sems.at[place],
            recv_sem=self.recv_sems.at[place],
            device_id=device,
            device_id_type=mesh_ids,
        )

    def start(self, name):
        self.copies[name].start()

    def arrived(self, name):
        self.copies[name].wait_recv()

    def finish(self):
        for copy in self.copies.values():
            copy.wait_send()


def greet(devices):
    barrier = pltpu.get_barrier_semaphore()
    for device in devices:
        pl.semaphore_signal(barrier, inc=1, device_id=device, device_id_type=mesh_ids)
    pl.semaphore_wait(barrier, len(devices))


def turned(index, step, size):
    return lax.rem(index + (step + size), size)


def whole_kernel(
    query_hbm, key_hbm, latent_hbm, weight_hbm, log_hbm, pair_hbm, cotangent_hbm, gain_hbm, lam_ref,
    dq_hbm, dk_hbm, dv_hbm, sum_hbm,
    query_all, grad_all, row_all, latent_all, key_all, value_all,
    dq_out, dk_out, dv_out, weight_out, maps, key_given, weight_ref, log_ref, pair_ref, cotangent_ref, gain_ref, value_own,
    dq_acc, dk_acc, dv_acc, dq_in, dq_stage, column_in, column_stage,
    mirror_stage, mirror_in, value_narrow,
    weight_part, weight_stage, weight_in, weight_mine, weight_last,
    local_sems, send_sems, recv_sems,
):
    z, x, y, core = (lax.axis_index(name) for name in ("z", "x", "y", "core"))
    group = jnp.where(z < 4, 0, 1)
    half = group
    own_slot = y * 2 + core

    loads = {}
    for place, (name, source, target) in enumerate(
        (
            ("latent", latent_hbm, latent_all.at[own_slot]),
            ("key", key_hbm.at[half], key_all.at[group, x]),
            ("given", key_hbm.at[1 - half], key_given),
            ("pair", pair_hbm, pair_ref),
            ("cotangent", cotangent_hbm, cotangent_ref),
            ("gain", gain_hbm, gain_ref),
            ("log", log_hbm, log_ref),
            ("query", query_hbm, query_all.at[z]),
            ("weight", weight_hbm, weight_ref),
        )
    ):
        loads[name] = pltpu.make_async_copy(source, target, local_sems.at[place])
        loads[name].start()

    others = [{"z": turned(z, hops, 8)} for hops in range(1, 8)]
    up, down, mirror = others[0], others[6], {"z": 7 - z}
    right, left = {"x": turned(x, 1, 4)}, {"x": turned(x, -1, 4)}
    ahead, behind = {"y": turned(y, 1, 4)}, {"y": turned(y, -1, 4)}
    partner = {"core": 1 - core}
    greet(others + [right, left, ahead, behind, partner])
    sender = Sender(send_sems, recv_sems)
    plan, start, arrived = sender.plan, sender.start, sender.arrived
    halves = (pl.ds(0, 256), pl.ds(256, 256))

    stores = {
        name: pltpu.make_async_copy(source, target, local_sems.at[9 + place])
        for place, (name, source, target) in enumerate(
            (
                ("dq0", dq_out.at[halves[0]], dq_hbm.at[halves[0]]),
                ("dq1", dq_out.at[halves[1]], dq_hbm.at[halves[1]]),
                ("dk", dk_out, dk_hbm),
                ("dv", dv_out, dv_hbm),
                ("weight", weight_out, sum_hbm),
            )
        )
    }

    def store(name):
        stores[name].start()

    def latent_slot(step, toks, part=None):
        slot = latent_all.at[turned(y, step, 4) * 2 + core, toks]
        return slot if part is None else slot.at[:, pl.ds(128 * part, 128)]

    sides = {"ahead": (ahead, -1, 0), "behind": (behind, 1, 1)}
    for name, toks in (("given", 1 - half), ("own", half)):
        for way, (device, step, far) in sides.items():
            for part in (0, 1):
                plan((name, way, part), latent_slot(0, toks, part), latent_slot(0, toks, part), device)
            plan((name, way, "far"), latent_slot(step, toks, far), latent_slot(step, toks, far), device)
        for step in (0, -1, 1, 2):
            plan(("pair", name, step), latent_slot(step, toks), latent_slot(step, toks), partner)
    for way, device, sign in (("up", up, -1), ("down", down, 1)):
        for hops in range(4):
            index = turned(z, sign * hops, 8)
            for part in (0, 1):
                if hops < 3 or (way == "up") == (part == 0):
                    slot = (query_all, grad_all)[part].at[index]
                    plan((way, hops, part), slot, slot, device)
            if hops < 3 or way == "up":
                plan((way, hops, "rows"), row_all.at[index], row_all.at[index], device)
    for name, given, target in (("key", key_given, key_all), ("value", value_own, value_all)):
        own, other = target.at[group, x], target.at[1 - group, x]
        plan((name, "mirror"), given, own, mirror)
        for way, device, step in (("right", right, -1), ("left", left, 1)):
            plan((name, "own", way), own, own, device)
            plan((name, "other", way), other, other, device)
        own, other = target.at[group, turned(x, -1, 4)], target.at[1 - group, turned(x, 1, 4)]
        plan((name, "own", "far"), own, own, right)
        plan((name, "other", "far"), other, other, left)
    for name, inbox, stages in (
        ("other value", column_in.at[0], column_stage.at[0]),
        ("own value", column_in.at[1], column_stage.at[1]),
        ("other key", column_in.at[2], column_stage.at[2]),
        ("own key", column_in.at[3], column_stage.at[3]),
        ("weight", weight_in, weight_stage),
    ):
        for number, (way, device) in enumerate((("right", right), ("left", left))):
            plan((name, way, 2, number), stages.at[number, 0], inbox.at[number, 2], device)
            plan((name, way, 1, 1 - number), stages.at[number, 1], inbox.at[number, 1 - number], device)
            plan((name, way, 1, number), stages.at[number, 2], inbox.at[number, number], device)
    for number in (0, 1):
        plan(("mirror back", number), mirror_stage.at[number], mirror_in.at[number], mirror)
    for number, (way, device) in enumerate((("up", up), ("down", down))):
        for hops in (4, 3, 2, 1):
            for part in (0, 1):
                if hops < 4 or part == number:
                    place = number, hops - 1, part
                    plan(("dq", way, hops, part), dq_stage.at[place], dq_in.at[place], device)
    for hops in range(1, 8):
        plan(("weight", hops), weight_mine.at[turned(z, hops, 8)], weight_last.at[hops - 1], others[hops - 1])

    def open_latents(name):
        for part in (0, 1):
            start((name, "ahead", part))
            start((name, "behind", 1 - part))
        start(("pair", name, 0))

    def latents_far(name):
        for way, (_, _, far) in sides.items():
            arrived((name, way, far))
            start((name, way, "far"))

    def latents_near(name):
        for way, (_, step, far) in sides.items():
            arrived((name, way, 1 - far))
            start(("pair", name, step))

    def latents_last(name):
        arrived((name, "ahead", "far"))
        arrived((name, "behind", "far"))
        start(("pair", name, 2))

    def values_of(name, toks):
        for step in (0, -1, 1, 2):
            arrived(("pair", name, step))
        total = jnp.zeros((256, 128), f32)
        for slot in range(8):
            total += jnp.dot(latent_all[slot, toks], weight_ref[slot], preferred_element_type=f32)
        return total.astype(bf16)

    def send_query(hops, part):
        for way in ("up", "down"):
            if (way, hops, part) in sender.copies:
                start((way, hops, part))
            if part == 1 and (way, hops, "rows") in sender.copies:
                start((way, hops, "rows"))

    def pass_query(hops, part):
        for way in ("up", "down"):
            if (way, hops, part) in sender.copies:
                arrived((way, hops, part))
                if (way, hops + 1, part) in sender.copies:
                    start((way, hops + 1, part))
            if part == 1 and (way, hops, "rows") in sender.copies:
                arrived((way, hops, "rows"))
                if (way, hops + 1, "rows") in sender.copies:
                    start((way, hops + 1, "rows"))

    def share_own(name):
        start((name, "own", "right"))
        start((name, "own", "left"))

    def share_mirrored(name):
        arrived((name, "mirror"))
        start((name, "other", "left"))
        start((name, "other", "right"))

    def share_far(name):
        arrived((name, "own", "right"))
        start((name, "own", "far"))
        arrived((name, "other", "left"))
        start((name, "other", "far"))

    def close_share(name):
        for which, way in (("own", "left"), ("other", "right"), ("own", "far"), ("other", "far")):
            arrived((name, which, way))

    loads["latent"].wait()
    open_latents("given")
    loads["key"].wait()
    loads["given"].wait()
    start(("key", "mirror"))
    share_own("key")
    loads["query"].wait()
    send_query(0, 0)

    for name in ("pair", "cotangent", "gain", "log"):
        loads[name].wait()
    lam = lam_ref[0]
    first_out, second_out = pair_ref[:, 0:128].astype(f32), pair_ref[:, 128:256].astype(f32)
    merged = first_out - lam * second_out
    inv_norm = lax.rsqrt(jnp.mean(merged * merged, axis=-1, keepdims=True) + norm_floor)
    scaled = cotangent_ref[...].astype(f32) * gain_ref[...]
    inner_dot = jnp.mean(scaled * merged, axis=-1, keepdims=True)
    out_grad = (inv_norm * scaled - merged * (inv_norm * inv_norm * inv_norm) * inner_dot).astype(bf16)
    grad_all[z] = out_grad
    wide = out_grad.astype(f32)
    first_term = jnp.sum(wide * first_out, axis=-1, keepdims=True)
    second_term = jnp.sum(wide * second_out, axis=-1, keepdims=True)
    lane = lax.broadcasted_iota(jnp.int32, (1, 128), 1)
    terms = jnp.where(lane == 0, first_term, second_term).T
    log_lam = jnp.log(jnp.full((1, 512), lam, f32)) * log2_e
    row_all[z, 2:4, :] = terms[0:2]
    row_all[z, 0:1, :] = log_ref[0:1, :] * log2_e
    row_all[z, 1:2, :] = log_ref[1:2, :] * log2_e - log_lam
    send_query(0, 1)

    dq_acc[...] = jnp.zeros_like(dq_acc)
    dk_acc[...] = jnp.zeros_like(dk_acc)
    dv_acc[...] = jnp.zeros_like(dv_acc)

    latents_far("given")
    open_latents("own")
    share_mirrored("key")
    pass_query(0, 0)
    latents_near("given")
    share_far("key")
    latents_last("given")
    loads["weight"].wait()
    latents_far("own")
    value_own[...] = values_of("given", 1 - half)
    start(("value", "mirror"))
    pass_query(0, 1)
    latents_near("own")
    close_share("key")

    first_lanes = lane < 64

    def split(value):
        zero = jnp.zeros_like(value)
        return jnp.where(first_lanes, value, zero), jnp.where(first_lanes, zero, value)

    def block_at(count):
        hops = (count + 1) // 2
        return turned(z, jnp.where(count % 2 == 1, -hops, hops), 8)

    def both_groups(block, work):
        def one(number, carry):
            own = number == 1
            part = jnp.where(own, group, 1 - group)
            row = jnp.where(own, z, 7 - z)
            slot = jnp.where(own, block + 1, block - 7 + z)
            pl.when(block >= row)(lambda: work(part, row, slot))
            return carry

        lax.fori_loop(0, 2, one, 0)

    def maps_tile(part, block, slot, masked):
        key_0, key_1 = split(key_all[part].reshape(1024, 128))
        for tok in range(0, 512, tok_len):
            toks = slice(tok, tok + tok_len)
            query, grad = query_all[block, toks], grad_all[block, toks]
            score_0 = lax.dot_general(key_0, query, rows_by_rows, preferred_element_type=f32)
            score_1 = lax.dot_general(key_1, query, rows_by_rows, preferred_element_type=f32)
            map_0 = jnp.exp2(score_0 * (log2_e / 8) - row_all[block, 0:1, toks])
            map_1 = jnp.exp2(score_1 * (log2_e / 8) - row_all[block, 1:2, toks])
            if masked:
                row = lax.broadcasted_iota(jnp.int32, (1024, 1), 0)
                key_pos = (row // 256 - x) * 512 + half * 256 + row % 256
                tok_pos = lax.broadcasted_iota(jnp.int32, (1, tok_len), 1) + tok
                visible = key_pos <= tok_pos
                map_0 = jnp.where(visible, map_0, 0.0)
                map_1 = jnp.where(visible, map_1, 0.0)
            maps[slot, 0, :, toks] = map_0.astype(bf16)
            maps[slot, 1, :, toks] = map_1.astype(bf16)
            mixed = (map_0 - map_1).astype(bf16)
            dv = lax.dot_general(mixed, grad, rows_by_cols, preferred_element_type=f32)
            dv_acc[part] += dv.reshape(4, 256, 128)

    def grads_tile(part, block, slot):
        key_0, key_1 = split(key_all[part].reshape(1024, 128))
        value = value_all[part].reshape(1024, 128)
        for tok in range(0, 512, tok_len):
            toks = slice(tok, tok + tok_len)
            query_0, query_1 = split(query_all[block, toks])
            dot = lax.dot_general(value, grad_all[block, toks], rows_by_rows, preferred_element_type=f32)
            map_0, map_1 = maps[slot, 0, :, toks].astype(f32), maps[slot, 1, :, toks].astype(f32)
            grad_0 = (map_0 * (dot - row_all[block, 2:3, toks])).astype(bf16)
            grad_1 = (map_1 * (row_all[block, 3:4, toks] - dot)).astype(bf16)
            dk = lax.dot_general(
                grad_0, query_0, rows_by_cols, preferred_element_type=f32
            ) + lax.dot_general(grad_1, query_1, rows_by_cols, preferred_element_type=f32)
            dk_acc[part] += dk.reshape(4, 256, 128)
            dq = lax.dot_general(
                key_0, grad_0, cols_by_cols, preferred_element_type=f32
            ) + lax.dot_general(key_1, grad_1, cols_by_cols, preferred_element_type=f32)
            dq_acc[block, toks, :] += dq.T

    def send_column(name, way, hops, part, pieces, inbox, stages):
        number, sign = (0, 1) if way == "right" else (1, -1)
        value = pieces(turned(x, sign * hops, 4), part)
        place = 0 if hops == 2 else 1
        if hops == 1 and part == number:
            arrived((name, way, 2, part))
            value += inbox[number, 2].astype(f32)
            place = 2
        stages[number, place] = value.astype(bf16)
        start((name, way, hops, part))

    def first_columns(name, *args):
        send_column(name, "right", 2, 0, *args)
        send_column(name, "left", 2, 1, *args)
        send_column(name, "right", 1, 1, *args)
        send_column(name, "left", 1, 0, *args)

    def last_columns(name, *args):
        send_column(name, "right", 1, 0, *args)
        send_column(name, "left", 1, 1, *args)

    def column_sum(name, part, pieces, inbox):
        arrived((name, "right", 1, part))
        arrived((name, "left", 1, part))
        return pieces(x, part) + inbox[0, part].astype(f32) + inbox[1, part].astype(f32)

    def sum_args(acc, rows_of, number):
        def pieces(j, part):
            return acc[rows_of, j, 128 * part : 128 * part + 128, :]

        return pieces, column_in.at[number], column_stage.at[number]

    other_value, own_value = sum_args(dv_acc, 1 - group, 0), sum_args(dv_acc, group, 1)
    other_key, own_key = sum_args(dk_acc, 1 - group, 2), sum_args(dk_acc, group, 3)
    weight_args = (lambda j, part: weight_part[j, 4 * part : 4 * part + 4]), weight_in, weight_stage

    def mirrored_rows(name, number, args):
        for part in (0, 1):
            mirror_stage[number, 128 * part : 128 * part + 128] = column_sum(name, part, *args[:2]).astype(bf16)
        start(("mirror back", number))

    def own_rows(name, args, out):
        for part in (0, 1):
            out[group, 128 * part : 128 * part + 128] = column_sum(name, part, *args[:2])

    def send_dq(way, hops, part):
        number, sign = (0, 1) if way == "up" else (1, -1)
        value = dq_acc[turned(z, sign * hops, 8), halves[part]]
        if hops < 3 or (hops == 3 and part == number):
            arrived(("dq", way, hops + 1, part))
            value += dq_in[number, hops, part].astype(f32)
        dq_stage[number, hops - 1, part] = value.astype(bf16)
        start(("dq", way, hops, part))

    def maps_step(count, carry):
        @pl.when(count == 1)
        def _():
            latents_last("own")
            value_all[group, x] = values_of("own", half)
            share_own("value")

        @pl.when(count == 2)
        def _():
            pass_query(1, 0)
            share_mirrored("value")

        @pl.when(count == 3)
        def _():
            pass_query(1, 1)
            share_far("value")

        pl.when(count == 4)(lambda: pass_query(2, 0))
        pl.when(count == 5)(lambda: pass_query(2, 1))

        @pl.when(count == 7)
        def _():
            pass_query(3, 0)
            pass_query(3, 1)

        block = block_at(count)

        def work(part, row, slot):
            pl.when(block == row)(lambda: maps_tile(part, block, slot, True))
            pl.when(block != row)(lambda: maps_tile(part, block, slot, False))

        both_groups(block, work)
        return carry

    lax.fori_loop(0, 8, maps_step, 0)
    first_columns("other value", *other_value)
    close_share("value")

    def weights_made():
        arrived(("mirror back", 0))
        value_narrow[1 - group] = mirror_in[0]
        dv_out[1 - group] = mirror_in[0].astype(f32)
        narrow = value_narrow[...].reshape(512, 128)
        for block in range(8):
            part = lax.dot_general(
                latent_all[block].reshape(512, 256), narrow, cols_by_cols, preferred_element_type=f32
            )
            weight_part[:, block] = part.reshape(4, 64, 128)
            if block == 3:
                send_column("weight", "right", 2, 0, *weight_args)
                send_column("weight", "left", 1, 0, *weight_args)
        send_column("weight", "left", 2, 1, *weight_args)
        send_column("weight", "right", 1, 1, *weight_args)

    def weights_summed():
        for part in (0, 1):
            weight_mine[4 * part : 4 * part + 4] = column_sum("weight", part, *weight_args[:2]).astype(bf16)
        for hops in (4, 3, 5, 2, 6, 1, 7):
            start(("weight", hops))

    def tile_at(count):
        found, passed = jnp.int32(0), jnp.int32(0)
        for row in (7 - z, z):
            for hops in (4, 3, 5, 2, 6, 1, 7, 0):
                block = turned(z, hops, 8)
                counts = block >= row
                found = jnp.where(counts & (passed == count), block, found)
                passed = passed + jnp.where(counts, 1, 0)
        return found

    def grads_step(count, carry):
        other = count <= z
        block = tile_at(count)
        part = jnp.where(other, 1 - group, group)
        grads_tile(part, block, jnp.where(other, block - 7 + z, block + 1))

        @pl.when(count == 1)
        def _():
            last_columns("other value", *other_value)
            first_columns("own value", *own_value)

        @pl.when(count == 3)
        def _():
            mirrored_rows("other value", 0, other_value)
            last_columns("own value", *own_value)

        @pl.when(count == 5)
        def _():
            send_dq("up", 4, 0)
            send_dq("down", 4, 1)
            send_dq("up", 3, 1)
            send_dq("down", 3, 0)
            own_rows("own value", own_value, dv_out)
            value_narrow[group] = dv_out[group].astype(bf16)

        pl.when(count == 6)(weights_made)

        @pl.when(count == 7)
        def _():
            send_dq("up", 3, 0)
            send_dq("down", 3, 1)
            send_dq("up", 2, 1)
            send_dq("down", 2, 0)

        pl.when(count == z)(lambda: first_columns("other key", *other_key))
        pl.when((count == z + 2) & (z < 6))(lambda: last_columns("other key", *other_key))
        pl.when((count == z + 4) & (z < 4))(lambda: mirrored_rows("other key", 1, other_key))
        return carry

    lax.fori_loop(0, 9, grads_step, 0)
    first_columns("own key", *own_key)
    store("dv")
    pl.when(z >= 6)(lambda: last_columns("other key", *other_key))
    last_columns("weight", *weight_args)
    send_dq("up", 2, 0)
    send_dq("down", 2, 1)
    send_dq("up", 1, 1)
    send_dq("down", 1, 0)
    last_columns("own key", *own_key)
    pl.when(z >= 4)(lambda: mirrored_rows("other key", 1, other_key))
    weights_summed()
    send_dq("up", 1, 0)
    send_dq("down", 1, 1)
    own_rows("own key", own_key, dk_out)
    arrived(("mirror back", 1))
    dk_out[1 - group] = mirror_in[1].astype(f32)
    store("dk")
    for part in (0, 1):
        arrived(("dq", "up", 1, part))
        arrived(("dq", "down", 1, part))
        dq_out[halves[part]] = (
            dq_acc[z, halves[part]] + dq_in[0, 0, part].astype(f32) + dq_in[1, 0, part].astype(f32)
        )
        store("dq" + str(part))
    total = weight_mine[z].astype(f32)
    for hops in range(1, 8):
        arrived(("weight", hops))
        total += weight_last[hops - 1].astype(f32)
    weight_out[...] = total
    store("weight")
    for copy in stores.values():
        copy.wait()
    sender.finish()


def finish_kernel(*refs):
    sums, outs, held, load_sems, store_sems = refs[:4], refs[4:8], refs[8:12], refs[12], refs[13]
    loads = [pltpu.make_async_copy(sums[i], held[i], load_sems.at[i]) for i in range(4)]
    stores = [pltpu.make_async_copy(held[i], outs[i], store_sems.at[i]) for i in range(4)]
    for load in loads:
        load.start()
    for i in (3, 2):
        loads[i].wait()
        stores[i].start()
    for i in (0, 1):
        loads[i].wait()
        held[i][...] = 0.125 * held[i][...]
        stores[i].start()
    for store in stores:
        store.wait()


def per_device(queries, key_vectors, latents, w_value, log_sums, out_pair, cotangent, lambdas, out_gain):
    anywhere = pl.BlockSpec(memory_space=pl.ANY)
    scratch = (
        ((8, 512, 128), bf16),
        ((8, 512, 128), bf16),
        ((8, 4, 512), f32),
        ((8, 2, 256, 256), bf16),
        ((2, 4, 256, 128), bf16),
        ((2, 4, 256, 128), bf16),
        ((512, 128), f32),
        ((2, 256, 128), f32),
        ((2, 256, 128), f32),
        ((64, 128), f32),
        ((9, 2, 1024, 512), bf16),
        ((256, 128), bf16),
        ((8, 256, 128), bf16),
        ((2, 512), f32),
        ((512, 256), bf16),
        ((512, 128), bf16),
        ((1, 128), f32),
        ((256, 128), bf16),
        ((8, 512, 128), f32),
        ((2, 4, 256, 128), f32),
        ((2, 4, 256, 128), f32),
        ((2, 4, 2, 256, 128), bf16),
        ((2, 4, 2, 256, 128), bf16),
        ((4, 2, 3, 128, 128), bf16),
        ((4, 2, 3, 128, 128), bf16),
        ((2, 256, 128), bf16),
        ((2, 256, 128), bf16),
        ((2, 256, 128), bf16),
        ((4, 8, 64, 128), f32),
        ((2, 3, 4, 64, 128), bf16),
        ((2, 3, 4, 64, 128), bf16),
        ((8, 64, 128), bf16),
        ((7, 64, 128), bf16),
    )
    sums = pl.pallas_call(
        whole_kernel,
        out_shape=(
            jax.ShapeDtypeStruct((512, 128), f32),
            jax.ShapeDtypeStruct((2, 256, 128), f32),
            jax.ShapeDtypeStruct((2, 256, 128), f32),
            jax.ShapeDtypeStruct((64, 128), f32),
        ),
        in_specs=[anywhere] * 8 + [pl.BlockSpec(memory_space=pltpu.SMEM)],
        out_specs=[anywhere] * 4,
        scratch_shapes=[pltpu.VMEM(*entry) for entry in scratch]
        + [
            pltpu.SemaphoreType.DMA((14,)),
            pltpu.SemaphoreType.DMA((116,)),
            pltpu.SemaphoreType.DMA((116,)),
        ],
        compiler_params=pltpu.CompilerParams(
            collective_id=0, has_side_effects=True, vmem_limit_bytes=60 * 1024 * 1024
        ),
        name="whole",
    )(
        queries,
        key_vectors.reshape(2, 256, 128),
        latents.reshape(2, 256, 256),
        w_value.reshape(8, 256, 128),
        log_sums.T,
        out_pair,
        cotangent,
        out_gain.reshape(1, 128),
        lambdas,
    )
    query_grad, key_grad, value_grad, weight_grad = pl.pallas_call(
        finish_kernel,
        out_shape=tuple(jax.ShapeDtypeStruct(part.shape, f32) for part in sums),
        in_specs=[anywhere] * 4,
        out_specs=[anywhere] * 4,
        scratch_shapes=[pltpu.VMEM(part.shape, f32) for part in sums]
        + [pltpu.SemaphoreType.DMA((4,)), pltpu.SemaphoreType.DMA((4,))],
        compiler_params=pltpu.CompilerParams(vmem_limit_bytes=60 * 1024 * 1024),
        name="finish",
    )(*sums)
    return query_grad, key_grad.reshape(512, 128), value_grad.reshape(512, 128), weight_grad


def solution(mesh):
    grid = Mesh(mesh.devices.reshape(8, 4, 4, 2), ("z", "x", "y", "core"))
    sp, tp = ("z", "x"), ("y", "core")
    return jax.shard_map(
        per_device,
        mesh=grid,
        in_specs=(
            P(sp, tp),
            P(sp, tp),
            P(sp, tp),
            P(None, tp),
            P(sp, tp),
            P(sp, tp),
            P(sp, tp),
            P(tp),
            P(),
        ),
        out_specs=(P(sp, tp), P(sp, tp), P(sp, tp), P(sp, tp)),
        check_vma=False,
    )
```
